256 devices in a mesh: sp: 32 (over z, x), tp: 8 (over y, core).
Axes of the slice: x: 4, y: 4, z: 8, core: 2. Of those that a mesh axis runs over, the one named last changes fastest.
Arguments:
- tokens: bfloat16 [32768, 2048], P('sp', 'tp'), may hold values from -70 to 70
- w_query: bfloat16 [2048, 1024], P(None, 'tp'), may hold values from -0.125 to 0.125
- w_key: bfloat16 [2048, 1024], P(None, 'tp'), may hold values from -0.125 to 0.125
- w_value: bfloat16 [2048, 1024], P(None, 'tp'), may hold values from -0.125 to 0.125
- w_delta_gate: bfloat16 [2048, 1024], P(None, 'tp'), may hold values from -0.125 to 0.125
- w_glu_value: bfloat16 [2048, 1024], P(None, 'tp'), may hold values from -0.125 to 0.125
- w_glu_gate: bfloat16 [2048, 1024], P(None, 'tp'), may hold values from -0.125 to 0.125
- w_conv_gate: bfloat16 [2048, 1024], P(None, 'tp'), may hold values from -0.125 to 0.125
- w_beta: bfloat16 [2048, 8], replicated, may hold values from -0.125 to 0.125
- w_decay: bfloat16 [2048, 8], replicated, may hold values from -0.125 to 0.125
- decay_log: float32 [8], replicated, may hold values from -12 to -3
- head_gain: float32 [128], replicated, may hold values from 0.1 to 1.9
- conv_taps: bfloat16 [31, 1024], P(None, 'tp'), may hold values from -2.5 to 2.5
- ln_gain: float32 [1024], P('tp'), may hold values from 0.1 to 1.9
- ln_shift: float32 [1024], P('tp'), may hold values from -3 to 3
- out_delta: bfloat16 [1024, 2048], P('tp'), may hold values from -0.125 to 0.125
- out_conv: bfloat16 [1024, 2048], P('tp'), may hold values from -0.125 to 0.125
Outputs:
- mixed_out: bfloat16 [32768, 2048], P(('sp', 'tp'))
The draws below stay inside these ranges and needn't reach their ends.
All inputs are finite; a program needn't handle non-finite values.
Results may differ from the reference program's by a relative error of at most 0.024.
Values may be sent and summed in bfloat16 or wider, within the bound.
A program may use at most 64 MiB of HBM per device.

```python
import jax
import jax.numpy as jnp
from jax import lax

D = 2048
HEADS = 8
DK = 128
CV = 1024
KERNEL = 31
SPAN = 64
TOKENS = 32768
N_TP = 8


def draw_tokens(key, part):
    keys = jax.random.split(key, 3)
    span_rows = 4 * SPAN
    groups = (TOKENS + span_rows - 1) // span_rows
    shifts = jnp.clip(jax.random.normal(keys[1], (groups, D), jnp.float32), -6.0, 6.0) * 1.5
    shifts = jnp.repeat(shifts, span_rows, axis=0)[:TOKENS]
    noise = jnp.clip(jax.random.normal(keys[0], (TOKENS, D), jnp.float32), -6.0, 6.0)
    spread = 0.7
    scales = jnp.exp(jax.random.uniform(keys[2], (TOKENS, 1), jnp.float32, -spread, spread))
    return ((noise + shifts) * scales).astype(jnp.bfloat16)


def draw_decay_log(key, part):
    keys = jax.random.split(key, 3)
    order = jax.random.permutation(keys[0], HEADS)
    fast_heads = HEADS // 2
    slow_rate = jax.random.uniform(keys[1], (HEADS,), jnp.float32, 0.3, 1.0) * 2.3 / TOKENS
    fast_rate = jax.random.uniform(keys[2], (HEADS,), jnp.float32, 0.015, 0.04)
    return jnp.log(jnp.where(order < fast_heads, fast_rate, slow_rate)).astype(jnp.float32)


def draw_conv_taps(key, part):
    keys = jax.random.split(key, 2)
    noise = jnp.clip(jax.random.normal(keys[0], (KERNEL, CV), jnp.float32), -4.0, 4.0)
    spread = 1.2
    levels = jnp.exp(jax.random.uniform(keys[1], (16,), jnp.float32, -spread, spread))
    group_ids = jnp.arange(CV) * 16 // CV
    column_scale = jnp.take(levels, group_ids)
    return (noise * column_scale[None, :] * KERNEL ** (-0.5)).astype(jnp.bfloat16)


def level_of(key, shape, shards, smallest, high):
    def one(axis_at, shards_of):
        heights = jax.random.uniform(jax.random.fold_in(jax.random.fold_in(key, 6), axis_at), (shards_of,), jnp.float32, smallest / len(shards), high / len(shards))
        return jnp.repeat(jnp.exp(heights), shape[axis_at] // shards_of).reshape((-1,) + (1,) * (len(shape) - axis_at - 1))

    loudness = one(*shards[0])
    for cut in shards[1:]:
        loudness = loudness * one(*cut)
    return loudness


def gaussian(own_key, shape, scale, reach, shards=(), kind=jnp.bfloat16):
    entries = scale * jax.random.normal(own_key, shape, jnp.float32)
    if shards:
        entries = entries * level_of(own_key, shape, shards, -0.22, 0.18)
    return jnp.clip(entries, -reach, reach).astype(kind)


def setup_inputs(seed: int = 0) -> dict:
    splits = jax.random.split(jax.random.key(seed), 18)
    tokens = draw_tokens(jax.random.fold_in(splits[17], 71), 0)
    w_query = gaussian(splits[1], (D, HEADS * DK), D ** -0.5, 0.125, ((1, 8),))
    w_key = gaussian(splits[2], (D, HEADS * DK), D ** -0.5, 0.125, ((1, 8),))
    w_value = gaussian(splits[3], (D, HEADS * DK), D ** -0.5, 0.125, ((1, 8),))
    w_delta_gate = gaussian(splits[4], (D, HEADS * DK), D ** -0.5, 0.125, ((1, 8),))
    w_glu_value = gaussian(splits[5], (D, CV), D ** -0.5, 0.125, ((1, 8),))
    w_glu_gate = gaussian(splits[6], (D, CV), D ** -0.5, 0.125, ((1, 8),))
    w_conv_gate = gaussian(splits[7], (D, CV), D ** -0.5, 0.125, ((1, 8),))
    w_beta = gaussian(splits[8], (D, HEADS), D ** -0.5, 0.125)
    w_decay = gaussian(splits[9], (D, HEADS), D ** -0.5, 0.125)
    decay_log = draw_decay_log(jax.random.fold_in(splits[17], 71), 0)
    head_gain = jnp.clip(1.0 + 0.18 * jax.random.normal(splits[11], (DK,), jnp.float32), 0.1, 1.9)
    conv_taps = draw_conv_taps(jax.random.fold_in(splits[17], 71), 0)
    ln_gain = jnp.clip(1.0 + 0.18 * jax.random.normal(splits[13], (CV,), jnp.float32), 0.1, 1.9)
    ln_shift = gaussian(splits[14], (CV,), 0.5, 3.0, ((0, 8),), jnp.float32)
    out_delta = gaussian(splits[15], (HEADS * DK, D), (HEADS * DK + CV) ** -0.5, 0.125, ((0, 8),))
    out_conv = gaussian(splits[16], (CV, D), (HEADS * DK + CV) ** -0.5, 0.125, ((0, 8),))
    return {"tokens": tokens, "w_query": w_query, "w_key": w_key, "w_value": w_value, "w_delta_gate": w_delta_gate, "w_glu_value": w_glu_value, "w_glu_gate": w_glu_gate, "w_conv_gate": w_conv_gate, "w_beta": w_beta, "w_decay": w_decay, "decay_log": decay_log, "head_gain": head_gain, "conv_taps": conv_taps, "ln_gain": ln_gain, "ln_shift": ln_shift, "out_delta": out_delta, "out_conv": out_conv}


TINY_NORM = 1e-06
TINY_VAR = 1e-05
HIGHEST = lax.Precision.HIGHEST

def head_rule(query, keys, values, strength, log_decay):
    blocks = query.shape[0] // SPAN

    def split_blocks(array):
        return array.reshape((blocks, SPAN) + array.shape[1:])
    query, keys, values = (split_blocks(query), split_blocks(keys), split_blocks(values))
    strength, log_decay = (split_blocks(strength), split_blocks(log_decay))
    log_sum = jnp.cumsum(log_decay, axis=-1)
    offsets = jnp.arange(SPAN)
    causal = offsets[:, None] >= offsets[None, :]
    strict = offsets[:, None] > offsets[None, :]
    spread = log_sum[:, :, None] - log_sum[:, None, :]
    damping = jnp.where(causal, jnp.exp(jnp.where(causal, spread, 0.0)), 0.0)
    scaled_keys = keys * strength[..., None]
    lower = jnp.where(strict, jnp.einsum('nid,njd->nij', scaled_keys, keys, precision=HIGHEST) * damping, 0.0)
    identity = jnp.eye(SPAN, dtype=jnp.float32)
    right = jnp.concatenate([values * strength[..., None], scaled_keys * jnp.exp(log_sum)[..., None]], axis=-1)
    solved = jax.scipy.linalg.solve_triangular(identity + lower, right, lower=True, unit_diagonal=True)
    width = values.shape[-1]
    corrected = solved[..., :width]
    key_terms = solved[..., width:]
    scores = jnp.einsum('nid,njd->nij', query, keys, precision=HIGHEST) * damping

    def advance(memory, inputs):
        query_block, keys_block, corrected_block, terms_block, scores_block, log_block = inputs
        fresh = corrected_block - jnp.dot(terms_block, memory, precision=HIGHEST)
        output = jnp.dot(query_block * jnp.exp(log_block)[:, None], memory, precision=HIGHEST)
        output = output + jnp.dot(scores_block, fresh, precision=HIGHEST)
        tail_log = log_block[-1]
        weighted = keys_block * jnp.exp(tail_log - log_block)[:, None]
        memory = memory * jnp.exp(tail_log) + jnp.dot(weighted.T, fresh, precision=HIGHEST)
        return (memory, output)
    start = jnp.zeros((keys.shape[-1], width), jnp.float32)
    ignored, outputs = lax.scan(advance, start, (query, keys, corrected, key_terms, scores, log_sum))
    return outputs.reshape(blocks * SPAN, width)

def reference(tokens, w_query, w_key, w_value, w_delta_gate, w_glu_value, w_glu_gate, w_conv_gate, w_beta, w_decay, decay_log, head_gain, conv_taps, ln_gain, ln_shift, out_delta, out_conv):
    length = tokens.shape[0]
    floats = tokens.astype(jnp.float32)
    inv_rms = lax.rsqrt(lax.optimization_barrier(jnp.mean(floats * floats, axis=1, keepdims=True)) + TINY_NORM)

    def project(weight):
        return jnp.dot(tokens.astype(jnp.float32), weight.astype(jnp.float32), preferred_element_type=jnp.float32) * inv_rms
    query_raw = project(w_query).astype(jnp.bfloat16)
    key_raw = project(w_key).astype(jnp.bfloat16)
    value_raw = project(w_value).astype(jnp.bfloat16)
    delta_gate_raw = project(w_delta_gate).astype(jnp.bfloat16)
    glu_value_raw = project(w_glu_value).astype(jnp.bfloat16)
    glu_gate_raw = project(w_glu_gate).astype(jnp.bfloat16)
    conv_gate_raw = project(w_conv_gate).astype(jnp.bfloat16)
    strength = jax.nn.sigmoid(project(w_beta))
    log_decay = -jnp.exp(decay_log)[None, :] * jax.nn.softplus(project(w_decay))

    def to_heads(raw):
        return raw.astype(jnp.float32).reshape(length, HEADS, DK)

    def unit_rows(array):
        return array * lax.rsqrt(lax.optimization_barrier(jnp.sum(array * array, axis=-1, keepdims=True)) + TINY_NORM)
    query = unit_rows(to_heads(query_raw)) * DK ** (-0.5)
    keys = unit_rows(to_heads(key_raw))
    values = to_heads(value_raw)
    heads_out = lax.map(lambda inputs: head_rule(*inputs), (jnp.moveaxis(query, 1, 0), jnp.moveaxis(keys, 1, 0), jnp.moveaxis(values, 1, 0), strength.T, log_decay.T))
    output = jnp.moveaxis(heads_out, 0, 1)
    output = output * lax.rsqrt(lax.optimization_barrier(jnp.mean(output * output, axis=-1, keepdims=True)) + TINY_NORM) * head_gain
    delta_mixed = (output.reshape(length, HEADS * DK) * jax.nn.silu(delta_gate_raw.astype(jnp.float32))).astype(jnp.bfloat16)
    gated_units = (glu_value_raw.astype(jnp.float32) * jax.nn.sigmoid(glu_gate_raw.astype(jnp.float32))).astype(jnp.bfloat16)
    padded = jnp.concatenate([jnp.zeros((KERNEL - 1, CV), jnp.bfloat16), gated_units], axis=0)
    filtered = jnp.zeros((length, CV), jnp.float32)
    for offset in range(KERNEL):
        filtered = filtered + padded[offset:offset + length].astype(jnp.float32) * conv_taps[offset].astype(jnp.float32)
    center = lax.optimization_barrier(jnp.sum(filtered, axis=1)) / CV
    variance = jnp.maximum(lax.optimization_barrier(jnp.sum(filtered * filtered, axis=1)) / CV - center * center, 0.0)
    normed = (filtered - center[:, None]) * lax.rsqrt(variance + TINY_VAR)[:, None] * ln_gain + ln_shift
    conv_mixed = (jax.nn.silu(normed) * jax.nn.silu(conv_gate_raw.astype(jnp.float32))).astype(jnp.bfloat16)
    head_block = HEADS * DK // N_TP
    chan_block = CV // N_TP
    summed = jnp.zeros((length, D), jnp.float32)
    for group in range(N_TP):
        partial_value = jnp.dot(delta_mixed[:, group * head_block:(group + 1) * head_block].astype(jnp.float32), out_delta[group * head_block:(group + 1) * head_block].astype(jnp.float32), preferred_element_type=jnp.float32)
        partial_value = partial_value + jnp.dot(conv_mixed[:, group * chan_block:(group + 1) * chan_block].astype(jnp.float32), out_conv[group * chan_block:(group + 1) * chan_block].astype(jnp.float32), preferred_element_type=jnp.float32)
        partial_value = lax.optimization_barrier(partial_value.astype(jnp.bfloat16))
        summed = summed + partial_value.astype(jnp.float32)
    return summed.astype(jnp.bfloat16)
```

```python
import jax
import jax.numpy as jnp
from jax import lax
from jax.experimental import pallas as pl
from jax.experimental.pallas import tpu as pltpu
from jax.sharding import PartitionSpec as P

BLOCK = 128
AHEAD = 3
TINY_NORM = 1e-06
TINY_VAR = 1e-05
HIGHEST = lax.Precision.HIGHEST
MESH = pl.DeviceIdType.MESH
F32 = jnp.float32
BF16 = jnp.bfloat16
NX = 4
NZ = 8
NY = 4


def nt(a, b):
    return lax.dot_general(a, b, (((1,), (1,)), ((), ())), preferred_element_type=F32)


def mm(a, b):
    return jnp.dot(a.astype(BF16), b.astype(BF16), preferred_element_type=F32)


def compose(later, earlier):
    width = later.shape[0]
    moved = mm(later[:, :width], earlier)
    return jnp.concatenate(
        [moved[:, :width], moved[:, width:] + later[:, width:].astype(F32)], axis=1
    )


def layer_kernel(
    tok_hbm, wq_hbm, wk_hbm, wv_hbm, wdg_hbm, wgv_hbm, wgg_hbm, wcg_hbm, wb_hbm, wdec_hbm,
    rate_hbm, gain_hbm, taps_hbm, lng_hbm, lns_hbm, od_hbm, oc_hbm,
    out_ref,
    full, w_all, proj, gates_ref, wb_s, wdec_s, rate_s, gain_s, taps_s, tapf_s, lng_s, lns_s,
    wd, wc, lhs_s, corr_s, score_s, wt_s, tail_s, state_ref, outa_s, outb_s,
    xin, zs, zr, zs4, zr4, padded, filtered, halo_out, halo_in, sums_out, sums_in,
    cm_s, dsend, in_d, in_c, acc, gate_s,
    l_sem, r_send, r_recv, l_send, l_recv, fr_send, fr_recv, fl_send, fl_recv,
    b_send, b_recv, w1_send, w1_recv, w2_send, w2_recv, w3_send, w3_recv, wb_send, wb_recv,
    wd_send, wd_recv, x_send, x_recv, z_send, z_recv, h_send, h_recv, ln_send, ln_recv,
    c_send, c_recv, d_send, d_recv,
):
    rows, part = tok_hbm.shape
    chunks = rows // BLOCK
    width = gain_hbm.shape[1]
    halo = halo_in.shape[0]
    kernel = taps_hbm.shape[0]
    sp, place = NX * NZ, lax.axis_index("sp")
    me = lax.axis_index("tp")
    core, y = lax.rem(me, 2), me // 2
    x, z = lax.rem(place, NX), place // NX
    sibling = me + 1 - 2 * core

    def tp_at(o, p=0):
        side = core + p * (1 - 2 * core)
        return lax.rem(y + o + NY, NY) * 2 + side

    def sp_at(dz, dx):
        return lax.rem(z + dz + NZ, NZ) * NX + lax.rem(x + dx + NX, NX)

    barrier = pltpu.get_barrier_semaphore()

    def greet(**device):
        pl.semaphore_signal(barrier, inc=1, device_id=device, device_id_type=MESH)

    for o in (1, 2, 3):
        for p in range(2):
            greet(tp=tp_at(o, p))
    greet(tp=sibling)
    for j in range(1, NZ):
        greet(sp=sp_at(j, 0))
    for k in range(1, NX):
        greet(sp=sp_at(0, k))
    greet(sp=lax.rem(place + sp - 1, sp))

    def columns(owner):
        return pl.ds(pl.multiple_of(owner * part, part), part)

    def at(t):
        return pl.ds(pl.multiple_of(t * BLOCK, BLOCK), BLOCK)

    def load(i, src, dst):
        return pltpu.make_async_copy(src, dst, l_sem.at[i])

    loads = {"tok": load(0, tok_hbm, full.at[:, columns(me)]), "oc": load(1, oc_hbm, wc.at[0, :BLOCK, :])}
    for i, src in enumerate((wq_hbm, wk_hbm, wv_hbm, wdg_hbm, wgv_hbm, wgg_hbm, wcg_hbm)):
        loads[i] = load(2 + i, src, w_all.at[:, i * width : (i + 1) * width])
    loads["wb"] = load(9, wb_hbm, wb_s)
    loads["wdec"] = load(10, wdec_hbm, wdec_s)
    loads["rate"] = load(11, rate_hbm, rate_s)
    loads["gain"] = load(12, gain_hbm, gain_s)
    loads["taps"] = load(13, taps_hbm, taps_s)
    loads["lng"] = load(14, lng_hbm, lng_s)
    loads["lns"] = load(15, lns_hbm, lns_s)
    loads["od"] = load(16, od_hbm, wd.at[0, :BLOCK, :])
    for copy in loads.values():
        copy.start()

    def remote(src, dst, send, recv, **device):
        return pltpu.make_async_remote_copy(
            src_ref=src, dst_ref=dst, send_sem=send, recv_sem=recv,
            device_id=device, device_id_type=MESH,
        )

    def to_right(r):
        block = full.at[at(r), columns(me)]
        return remote(block, block, r_send.at[r], r_recv.at[r], tp=tp_at(1))

    def to_left(r):
        block = full.at[at(r), columns(me)]
        return remote(block, block, l_send.at[r], l_recv.at[r], tp=tp_at(-1))

    def half(r, i):
        return pl.ds(pl.multiple_of(r * BLOCK + i * (BLOCK // 2), BLOCK // 2), BLOCK // 2)

    def on_right(r):
        block = full.at[half(r, 0), columns(tp_at(-1))]
        return remote(block, block, fr_send.at[r], fr_recv.at[r], tp=tp_at(1))

    def on_left(r):
        block = full.at[half(r, 1), columns(tp_at(1))]
        return remote(block, block, fl_send.at[r], fl_recv.at[r], tp=tp_at(-1))

    def beside(o, r):
        block = full.at[at(r), columns(tp_at(o))]
        return remote(block, block, b_send.at[o, r], b_recv.at[o, r], tp=sibling)

    zrows = BLOCK // NZ
    xcols = wc.shape[2] // NX

    def wpiece(i):
        return (
            pl.ds(pl.multiple_of(lax.rem(z - i + NZ, NZ) * zrows, zrows), zrows),
            pl.ds(pl.multiple_of(x * xcols, xcols), xcols),
        )

    def w_first(o):
        a, b = wpiece(0)
        return remote(
            wc.at[0, a, b], wc.at[NY - o, a, b], w1_send.at[o - 1], w1_recv.at[o - 1], tp=tp_at(o)
        )

    def w_second(j):
        a, b = wpiece(0)
        block = wc.at[pl.ds(1, NY - 1), a, b]
        return remote(block, block, w2_send.at[j - 1], w2_recv.at[j - 1], sp=sp_at(j, 0))

    def w_third(i, k):
        a, b = wpiece(i)
        block = wc.at[pl.ds(1, NY - 1), a, b]
        return remote(block, block, w3_send.at[i, k - 1], w3_recv.at[i, k - 1], sp=sp_at(0, k))

    def w_beside(i, ref):
        return remote(
            ref.at[:, pl.ds(0, BLOCK), :], ref.at[:, pl.ds(BLOCK, BLOCK), :],
            wb_send.at[i], wb_recv.at[i], tp=sibling,
        )

    hb = BLOCK // 2

    def d_right(i):
        return remote(
            wd.at[0, pl.ds(i * hb, hb), :], wd.at[3, pl.ds(i * hb, hb), :],
            wd_send.at[i], wd_recv.at[i], tp=tp_at(1),
        )

    def d_left(i):
        return remote(
            wd.at[0, pl.ds((1 - i) * hb, hb), :], wd.at[1, pl.ds((1 - i) * hb, hb), :],
            wd_send.at[2 + i], wd_recv.at[2 + i], tp=tp_at(-1),
        )

    def d_on_right():
        return remote(
            wd.at[3, pl.ds(0, hb), :], wd.at[2, pl.ds(0, hb), :],
            wd_send.at[4], wd_recv.at[4], tp=tp_at(1),
        )

    def d_on_left():
        return remote(
            wd.at[1, pl.ds(hb, hb), :], wd.at[2, pl.ds(hb, hb), :],
            wd_send.at[5], wd_recv.at[5], tp=tp_at(-1),
        )

    loads["tok"].wait()
    loads["oc"].wait()
    pl.semaphore_wait(barrier, 7 + NZ - 1 + NX - 1 + 1)
    for o in (2, 1, 3):
        w_first(o).start()
    for r in range(AHEAD):
        to_right(r).start()
        to_left(r).start()

    def own_beside(r, carry):
        beside(0, r).start()
        return carry

    lax.fori_loop(0, chunks, own_beside, 0)

    loads["wb"].wait()
    loads["wdec"].wait()
    loads["rate"].wait()
    heads = wb_s.shape[0]
    pick = lax.broadcasted_iota(jnp.int32, wb_s.shape, 0) == me
    beta_row = jnp.sum(jnp.where(pick, wb_s[...].astype(F32), 0.0), axis=0, keepdims=True)
    decay_row = jnp.sum(jnp.where(pick, wdec_s[...].astype(F32), 0.0), axis=0, keepdims=True)
    sub_id = lax.broadcasted_iota(jnp.int32, (BLOCK, BLOCK), 0)
    for b in range(2 * NY * part // BLOCK):
        cut = slice(b * BLOCK, (b + 1) * BLOCK)
        tall = jnp.where(sub_id == 0, beta_row[:, cut], jnp.where(sub_id == 1, decay_row[:, cut], 0.0))
        w_all[cut, 7 * width : 8 * width] = tall.T.astype(BF16)
    lane8 = lax.broadcasted_iota(jnp.int32, (1, heads), 1)
    rate = jnp.exp(
        jnp.sum(jnp.where(lane8 == me, rate_s[...], 0.0), axis=1, keepdims=True)
    )
    for i in range(7):
        loads[i].wait()
    loads["taps"].wait()
    tapf_s[:kernel, :] = taps_s[...].astype(F32)

    def arrive(r):
        to_right(r).wait_recv()
        to_left(r).wait_recv()
        on_right(r).start()
        on_left(r).start()
        beside(3, r).start()
        beside(1, r).start()

        @pl.when(r + AHEAD < chunks)
        def _():
            to_right(r + AHEAD).start()
            to_left(r + AHEAD).start()

    def arrive_far(r):
        on_right(r).wait_recv()
        on_left(r).wait_recv()
        beside(2, r).start()

    def w_pass(r):
        w_second(r).wait_recv()
        for k in (2, 1, 3):
            w_third(r, k).start()

    def chunk(r):
        for o in range(NY):
            beside(o, r).wait_recv()
        here = at(r)
        squares = jnp.zeros((BLOCK, 1), F32)
        for b in range(2 * NY):
            piece = full[here, b * part : (b + 1) * part].astype(F32)
            squares = squares + jnp.sum(piece * piece, axis=1, keepdims=True)
        inv_rms = lax.rsqrt(squares / (part * 2 * NY) + TINY_NORM)
        for j in range(4):
            summed = jnp.dot(
                full[here, :], w_all[:, j * 256 : (j + 1) * 256], preferred_element_type=F32
            )
            summed = summed * inv_rms
            proj[2 * j, here, :] = summed[:, :width].astype(BF16)
            if j < 3:
                proj[2 * j + 1, here, :] = summed[:, width:].astype(BF16)
            else:
                raw = summed[:, width:]
                lane = lax.broadcasted_iota(jnp.int32, raw.shape, 1)
                softplus = jnp.maximum(raw, 0.0) + jnp.log1p(jnp.exp(-jnp.abs(raw)))
                gates_ref[here, :] = jnp.where(
                    lane == 0, jax.nn.sigmoid(raw), jnp.where(lane == 1, -rate * softplus, 0.0)
                )

    row_id = lax.broadcasted_iota(jnp.int32, (BLOCK, BLOCK), 0)
    col_id = lax.broadcasted_iota(jnp.int32, (BLOCK, BLOCK), 1)
    causal = row_id >= col_id
    strict = row_id > col_id
    differ = row_id ^ col_id
    eye = jnp.where(row_id == col_id, 1.0, 0.0)
    tril = jnp.where(causal, 1.0, 0.0)
    ident = jnp.concatenate([eye, jnp.zeros((width, width), F32)], axis=1)

    def prepare(c):
        here = slice(c * BLOCK, (c + 1) * BLOCK)
        gates = gates_ref[here, :]
        sums = jnp.dot(tril, gates, precision=HIGHEST, preferred_element_type=F32)
        q, k = proj[0, here, :], proj[1, here, :]
        v = proj[2, here, :].astype(F32)
        kf, qf = k.astype(F32), q.astype(F32)
        ik = lax.rsqrt(jnp.sum(kf * kf, axis=-1, keepdims=True) + TINY_NORM)
        iq = lax.rsqrt(jnp.sum(qf * qf, axis=-1, keepdims=True) + TINY_NORM)
        iq = iq * width ** (-0.5)
        beta = gates[:, 0:1]
        log_sum = sums[:, 1:2]
        log_full = jnp.broadcast_to(log_sum, (BLOCK, BLOCK))
        spread = log_full - log_full.T
        damp = jnp.where(causal, jnp.exp(jnp.where(causal, spread, 0.0)), 0.0)
        damp = damp * jnp.broadcast_to(ik, (BLOCK, BLOCK)).T
        lower = jnp.where(strict, nt(k, k) * damp * (beta * ik), 0.0)
        score_s[here, :] = (nt(q, k) * damp * iq).astype(BF16)
        grow = jnp.exp(log_sum)
        right = jnp.concatenate([v * beta, kf * (beta * ik * grow)], axis=1)
        tail = log_full[BLOCK - 1 : BLOCK, :]
        weighted = kf * (ik * jnp.exp(tail[:, :1] - log_sum))
        wt_s[c] = weighted.T.astype(BF16)
        tail_s[c] = jnp.broadcast_to(jnp.exp(tail), (8, BLOCK))
        lhs_s[c, BLOCK:, :] = (qf * (iq * grow)).astype(BF16)
        return [c, lower, right, eye - jnp.where(differ == 1, lower, 0.0)]

    def advance(c, carry):
        both = mm(lhs_s[c], state_ref[...])
        first = both[:BLOCK]
        fresh = jnp.concatenate(
            [-first[:, :width], corr_s[at(c), :] - first[:, width:]], axis=1
        ).astype(BF16)
        decay = tail_s[c][:1, :]
        decay = jnp.concatenate([decay, decay], axis=1)
        state_ref[...] = state_ref[...] * decay + mm(wt_s[c], fresh)
        out = both[BLOCK:] + mm(score_s[at(c), :], fresh)
        outa_s[at(c), :] = out[:, :width].astype(BF16)
        outb_s[at(c), :] = out[:, width:]
        return carry

    def delta_group(first, count):
        chains = [prepare(first + i) for i in range(count)]
        size = 2
        while size < BLOCK:
            level = (differ >= size) & (differ < 2 * size)
            moved = [mm(jnp.where(level, ch[1], 0.0), ch[3]) for ch in chains]
            for ch, part_ in zip(chains, moved):
                ch[3] = ch[3] - mm(ch[3], part_)
            size *= 2
        for c, lower, right, inverse in chains:
            solved = mm(inverse, right)
            corr_s[c * BLOCK : (c + 1) * BLOCK, :] = solved[:, :width]
            lhs_s[c, :BLOCK, :] = solved[:, width:].astype(BF16)
        lax.fori_loop(first, first + count, advance, 0)

    state_ref[...] = ident
    for o in (1, 2, 3):
        w_first(o).wait_recv()
    for j in range(1, NZ):
        w_second(j).start()
    for k in (2, 1, 3):
        w_third(0, k).start()
    arrive(0)
    arrive(1)
    arrive_far(0)
    w_pass(1)

    def steady(r, carry):
        arrive(r)
        arrive_far(r - 1)
        chunk(r - 2)
        w_pass(r)
        return carry

    lax.fori_loop(2, 6, steady, 0)
    arrive(6)
    arrive_far(5)
    delta_group(0, 4)
    w_pass(6)
    arrive(7)
    arrive_far(6)
    loads["od"].wait()
    d_right(0).start()
    d_left(0).start()
    w_pass(7)

    def late(r, carry):
        @pl.when(r == 6)
        def _():
            arrive_far(7)

        chunk(r)
        return carry

    lax.fori_loop(4, 8, late, 0)

    def unit(t):
        value = proj[4, at(t), :].astype(F32)
        units = (value * jax.nn.sigmoid(proj[5, at(t), :].astype(F32))).astype(BF16)
        padded[pl.ds(pl.multiple_of(t * BLOCK + halo, halo), BLOCK), :] = units.astype(F32)
        return units

    units = unit(chunks - 1)
    halo_out[...] = units[BLOCK - halo :, :]
    halo_copy = remote(
        halo_out, halo_in, h_send.at[0], h_recv.at[0], sp=lax.rem(place + 1, sp)
    )

    @pl.when(place + 1 < sp)
    def _():
        halo_copy.start()

    delta_group(4, 4)

    xin[0] = state_ref[...].astype(BF16)

    def x_copy(k):
        return remote(xin.at[0], xin.at[k], x_send.at[k - 1], x_recv.at[k - 1], sp=sp_at(0, k))

    for k in (2, 1, 3):
        x_copy(k).start()

    def unit_loop(t, carry):
        unit(t)
        return carry

    lax.fori_loop(0, chunks - 1, unit_loop, 0)

    def conv(t, carry):
        total = jnp.zeros((BLOCK, width), F32)
        for j in range(kernel):
            start = t * BLOCK + (halo - kernel + 1 + j)
            total = total + padded[pl.ds(start, BLOCK), :] * tapf_s[j : j + 1, :]
        filtered[at(t), :] = total
        first = jnp.sum(total, axis=1, keepdims=True)
        second = jnp.sum(total * total, axis=1, keepdims=True)
        turned = jnp.where(col_id == 0, first, jnp.where(col_id == 1, second, 0.0)).T
        sums_out[pl.ds(t, 1), :] = turned[0:1, :]
        sums_out[pl.ds(t + 8, 1), :] = turned[1:2, :]
        return carry

    lax.fori_loop(1, chunks, conv, 0)

    for k in (1, 2, 3):
        x_copy(k).wait_recv()

    def piece(i):
        return xin[lax.rem(x - i + NX, NX)]

    p0, p1, p2, p3 = (piece(i) for i in range(NX))
    w2 = compose(p1, p0)
    pair = compose(p3, p2)
    group = compose(pair, w2)
    w3 = compose(p2, w2)
    inner = jnp.where(
        x == 0, ident, jnp.where(x == 1, p0.astype(F32), jnp.where(x == 2, w2, w3))
    ).astype(BF16)
    zs[0] = group.astype(BF16)

    def z_copy(i):
        return remote(zs.at[i], zr.at[i], z_send.at[i], z_recv.at[i], sp=sp_at(i + 1, 0))

    last_copy = remote(zs4, zr4, z_send.at[2], z_recv.at[2], sp=sp_at(4, 0))

    @pl.when(z + 1 < NZ)
    def _():
        z_copy(0).start()

    for i in range(2):

        @pl.when(z < i + 1)
        def _(i=i):
            zr[i] = ident.astype(BF16)

    @pl.when(z < 4)
    def _():
        zr4[...] = jnp.zeros(zr4.shape, BF16)

    @pl.when(place >= 1)
    def _():
        halo_copy.wait_recv()

    @pl.when(place < 1)
    def _():
        halo_in[...] = jnp.zeros(halo_in.shape, BF16)

    padded[:halo, :] = halo_in[...].astype(F32)
    conv(0, 0)

    def ln_copy(o, p):
        i = 2 * o + p - 1
        return remote(
            sums_out, sums_in.at[i], ln_send.at[i], ln_recv.at[i], tp=tp_at(o, p)
        )

    others = [(2, 0), (2, 1), (1, 0), (1, 1), (3, 0), (3, 1), (0, 1)]
    for o, p in others:
        ln_copy(o, p).start()
    d_right(1).start()
    d_left(1).start()

    @pl.when(z >= 1)
    def _():
        z_copy(0).wait_recv()

    e1 = zr[0]
    i2 = compose(zs[0], e1)
    zs[1] = i2.astype(BF16)

    @pl.when(z + 2 < NZ)
    def _():
        z_copy(1).start()

    for o, p in others:
        ln_copy(o, p).wait_recv()
    loads["lng"].wait()
    loads["lns"].wait()
    loads["gain"].wait()
    sums = sums_out[...]
    for i in range(7):
        sums = sums + sums_in[i]
    sums = jnp.concatenate([sums, jnp.zeros((BLOCK - 16, BLOCK), F32)], axis=0).T
    channels = width * 2 * NY
    center_all = sums[:, 0:8] / channels
    variance = jnp.maximum(sums[:, 8:16] / channels - center_all * center_all, 0.0)
    scale_all = lax.rsqrt(variance + TINY_VAR)
    for t in range(chunks):
        here = slice(t * BLOCK, (t + 1) * BLOCK)
        normed = (filtered[here, :] - center_all[:, t : t + 1]) * scale_all[:, t : t + 1]
        normed = normed * lng_s[...] + lns_s[...]
        gate = proj[6, here, :].astype(F32)
        cm_s[here, :] = (jax.nn.silu(normed) * jax.nn.silu(gate)).astype(BF16)

    def c_copy(o, p):
        i = 2 * o + p - 1
        return remote(
            cm_s.at[at(tp_at(o, p)), :],
            in_c.at[(NY - o) % NY, :, pl.ds(p * width, width)],
            c_send.at[i], c_recv.at[i], tp=tp_at(o, p),
        )

    for o, p in others:
        c_copy(o, p).start()
    in_c[0, :, :width] = cm_s[at(me), :]
    for i in range(NZ):
        for k in range(1, NX):
            w_third(i, k).wait_recv()
    w_beside(0, wc).start()

    @pl.when(z >= 2)
    def _():
        z_copy(1).wait_recv()

    n2 = zr[1]
    i2b = zs[1]
    zs4[...] = (mm(i2b[:, :width], n2[:, width:]) + i2b[:, width:].astype(F32)).astype(BF16)

    @pl.when(z + 4 < NZ)
    def _():
        last_copy.start()

    e3 = compose(e1, n2)
    reach = compose(inner, e3)
    d_right(0).wait_recv()
    d_left(0).wait_recv()
    d_on_right().start()
    d_on_left().start()

    for t in range(chunks):
        here = slice(t * BLOCK, (t + 1) * BLOCK)
        gate_s[here, :] = gain_s[...] * jax.nn.silu(proj[3, here, :].astype(F32))

    w_beside(0, wc).wait_recv()
    for o, p in others:
        c_copy(o, p).wait_recv()
    step = 512
    for n in range(out_ref.shape[1] // step):
        cut = slice(n * step, (n + 1) * step)
        total = jnp.zeros((BLOCK, step), F32)
        for d in range(NY):
            total = total + jnp.dot(in_c[d], wc[d, :, cut], preferred_element_type=F32)
        acc[:, cut] = total

    @pl.when(z >= 4)
    def _():
        last_copy.wait_recv()

    carried = (mm(reach[:, :width], zr4[...]) + reach[:, width:]).astype(BF16)

    def d_copy(o, p):
        i = 2 * o + p - 1
        return remote(
            dsend.at[i], in_d.at[(NY - o) % NY, :, pl.ds(p * width, width)],
            d_send.at[i], d_recv.at[i], tp=tp_at(o, p),
        )

    for batch in (others[:2], others[2:6], [(0, 1), (0, 0)]):
        places = [at(tp_at(o, p)) for o, p in batch]
        results = [outb_s[pos, :] + mm(outa_s[pos, :], carried) for pos in places]
        scales = [
            lax.rsqrt(jnp.mean(res * res, axis=-1, keepdims=True) + TINY_NORM) for res in results
        ]
        mixed = [
            (res * sc * gate_s[pos, :]).astype(BF16)
            for res, sc, pos in zip(results, scales, places)
        ]
        for (o, p), value in zip(batch, mixed):
            if o == 0 and p == 0:
                in_d[0, :, :width] = value
            else:
                dsend[2 * o + p - 1] = value
        for o, p in batch:
            if o or p:
                d_copy(o, p).start()

    d_right(1).wait_recv()
    d_left(1).wait_recv()
    d_on_right().wait_recv()
    d_on_left().wait_recv()
    w_beside(1, wd).start()
    w_beside(1, wd).wait_recv()
    for group_at in ((0,), (3, 1), (2,)):
        for d in group_at:
            o = (NY - d) % NY
            for p in range(2):
                if o or p:
                    d_copy(o, p).wait_recv()
        for n in range(out_ref.shape[1] // step):
            cut = slice(n * step, (n + 1) * step)
            total = acc[:, cut]
            for d in group_at:
                total = total + jnp.dot(in_d[d], wd[d, :, cut], preferred_element_type=F32)
            if group_at == (2,):
                out_ref[:, cut] = total.astype(BF16)
            else:
                acc[:, cut] = total

    def drain(r, carry):
        to_right(r).wait_send()
        to_left(r).wait_send()
        on_right(r).wait_send()
        on_left(r).wait_send()
        for o in range(NY):
            beside(o, r).wait_send()
        for k in range(1, NX):
            w_third(r, k).wait_send()
        return carry

    lax.fori_loop(0, chunks, drain, 0)
    for o in (1, 2, 3):
        w_first(o).wait_send()
    for j in range(1, NZ):
        w_second(j).wait_send()
    for i in range(2):
        d_right(i).wait_send()
        d_left(i).wait_send()
    d_on_right().wait_send()
    d_on_left().wait_send()
    w_beside(0, wc).wait_send()
    w_beside(1, wd).wait_send()
    for k in (1, 2, 3):
        x_copy(k).wait_send()

    @pl.when(place + 1 < sp)
    def _():
        halo_copy.wait_send()

    for i in range(2):

        @pl.when(z + i + 1 < NZ)
        def _(i=i):
            z_copy(i).wait_send()

    @pl.when(z + 4 < NZ)
    def _():
        last_copy.wait_send()

    for o, p in others:
        ln_copy(o, p).wait_send()
        c_copy(o, p).wait_send()
        d_copy(o, p).wait_send()


def local(
    tokens, w_query, w_key, w_value, w_delta_gate, w_glu_value, w_glu_gate, w_conv_gate,
    w_beta, w_decay, decay_log, head_gain, conv_taps, ln_gain, ln_shift, out_delta, out_conv,
):
    rows, part = tokens.shape
    depth, width = w_query.shape
    wide = out_delta.shape[1]
    heads = w_beta.shape[1]
    chunks = rows // BLOCK
    kernel = conv_taps.shape[0]
    halo = (kernel - 1 + 31) // 32 * 32
    hbm = pl.BlockSpec(memory_space=pltpu.HBM)
    dma = pltpu.SemaphoreType.DMA
    vm = pltpu.VMEM
    return pl.pallas_call(
        layer_kernel,
        out_shape=jax.ShapeDtypeStruct((BLOCK, wide), BF16),
        in_specs=[hbm] * 17,
        out_specs=pl.BlockSpec(memory_space=pltpu.VMEM),
        scratch_shapes=[
            vm((rows, depth), BF16),
            vm((depth, 8 * width), BF16),
            vm((7, rows, width), BF16),
            vm((rows, width), F32),
            vm((heads, depth), BF16),
            vm((heads, depth), BF16),
            vm((1, heads), F32),
            vm((1, width), F32),
            vm((kernel, width), BF16),
            vm((32, width), F32),
            vm((1, width), F32),
            vm((1, width), F32),
            vm((NY, 2 * BLOCK, wide), BF16),
            vm((NY, 2 * BLOCK, wide), BF16),
            vm((chunks, 2 * BLOCK, width), BF16),
            vm((rows, width), F32),
            vm((rows, BLOCK), BF16),
            vm((chunks, width, BLOCK), BF16),
            vm((chunks, 8, BLOCK), F32),
            vm((width, 2 * width), F32),
            vm((rows, width), BF16),
            vm((rows, width), F32),
            vm((NX, width, 2 * width), BF16),
            vm((2, width, 2 * width), BF16),
            vm((2, width, 2 * width), BF16),
            vm((width, width), BF16),
            vm((width, width), BF16),
            vm((halo + rows, width), F32),
            vm((rows, width), F32),
            vm((halo, width), BF16),
            vm((halo, width), BF16),
            vm((16, BLOCK), F32),
            vm((7, 16, BLOCK), F32),
            vm((rows, width), BF16),
            vm((7, BLOCK, width), BF16),
            vm((NY, BLOCK, 2 * width), BF16),
            vm((NY, BLOCK, 2 * width), BF16),
            vm((BLOCK, wide), F32),
            vm((rows, width), F32),
            dma((17,)),
            dma((chunks,)), dma((chunks,)), dma((chunks,)), dma((chunks,)),
            dma((chunks,)), dma((chunks,)), dma((chunks,)), dma((chunks,)),
            dma((NY, chunks)), dma((NY, chunks)),
            dma((NY - 1,)), dma((NY - 1,)),
            dma((NZ - 1,)), dma((NZ - 1,)),
            dma((NZ, NX - 1)), dma((NZ, NX - 1)),
            dma((2,)), dma((2,)),
            dma((6,)), dma((6,)),
            dma((NX - 1,)), dma((NX - 1,)),
            dma((3,)), dma((3,)),
            dma((1,)), dma((1,)),
            dma((7,)), dma((7,)),
            dma((7,)), dma((7,)),
            dma((7,)), dma((7,)),
        ],
        compiler_params=pltpu.CompilerParams(
            collective_id=0, has_side_effects=True, vmem_limit_bytes=60 * 1024 * 1024
        ),
        cost_estimate=pl.CostEstimate(
            flops=10_000_000_000, bytes_accessed=20_000_000, transcendentals=0
        ),
        name="layer",
    )(
        tokens, w_query, w_key, w_value, w_delta_gate, w_glu_value, w_glu_gate, w_conv_gate,
        w_beta.T, w_decay.T, decay_log[None, :], head_gain[None, :], conv_taps,
        ln_gain[None, :], ln_shift[None, :], out_delta, out_conv,
    )


def solution(mesh):
    return jax.shard_map(
        local,
        mesh=mesh,
        in_specs=(
            P("sp", "tp"), P(None, "tp"), P(None, "tp"), P(None, "tp"), P(None, "tp"),
            P(None, "tp"), P(None, "tp"), P(None, "tp"), P(), P(), P(), P(), P(None, "tp"),
            P("tp"), P("tp"), P("tp", None), P("tp", None),
        ),
        out_specs=P(("sp", "tp"), None),
        check_vma=False,
    )
```

```python
import jax
import jax.numpy as jnp
from jax import lax
from jax.experimental import pallas as pl
from jax.experimental.pallas import tpu as pltpu
from jax.sharding import PartitionSpec as P

BLOCK = 128
AHEAD = 3
TINY_NORM = 1e-06
TINY_VAR = 1e-05
HIGHEST = lax.Precision.HIGHEST
MESH = pl.DeviceIdType.MESH
F32 = jnp.float32
BF16 = jnp.bfloat16
NX = 4
NZ = 8
NY = 4


def nt(a, b):
    return lax.dot_general(a, b, (((1,), (1,)), ((), ())), preferred_element_type=F32)


def mm(a, b):
    return jnp.dot(a.astype(BF16), b.astype(BF16), preferred_element_type=F32)


def compose(later, earlier):
    width = later.shape[0]
    moved = mm(later[:, :width], earlier)
    return jnp.concatenate(
        [moved[:, :width], moved[:, width:] + later[:, width:].astype(F32)], axis=1
    )


def layer_kernel(
    tok_hbm, wq_hbm, wk_hbm, wv_hbm, wdg_hbm, wgv_hbm, wgg_hbm, wcg_hbm, wb_hbm, wdec_hbm,
    rate_hbm, gain_hbm, taps_hbm, lng_hbm, lns_hbm, od_hbm, oc_hbm,
    out_hbm,
    out_ref, full, w_all, proj, gates_ref, wb_s, wdec_s, rate_s, gain_s, taps_s, tapf_s, lng_s, lns_s,
    wd, wc, lhs_s, corr_s, score_s, wt_s, tail_s, state_ref, outa_s, outb_s,
    xin, zs, zr, zs4, zr4, padded, filtered, halo_out, halo_in, sums_out, sums_in,
    cm_s, dsend, in_d, in_c, acc, gate_s,
    l_sem, r_send, r_recv, l_send, l_recv, fr_send, fr_recv, fl_send, fl_recv,
    b_send, b_recv, w1_send, w1_recv, w2_send, w2_recv, w3_send, w3_recv, wb_send, wb_recv,
    wd_send, wd_recv, x_send, x_recv, z_send, z_recv, h_send, h_recv, ln_send, ln_recv,
    c_send, c_recv, d_send, d_recv, o_sem,
):
    rows, part = tok_hbm.shape
    chunks = rows // BLOCK
    width = gain_hbm.shape[1]
    halo = halo_in.shape[0]
    kernel = taps_hbm.shape[0]
    sp, place = NX * NZ, lax.axis_index("sp")
    me = lax.axis_index("tp")
    core, y = lax.rem(me, 2), me // 2
    x, z = lax.rem(place, NX), place // NX
    sibling = me + 1 - 2 * core

    def tp_at(o, p=0):
        side = core + p * (1 - 2 * core)
        return lax.rem(y + o + NY, NY) * 2 + side

    def sp_at(dz, dx):
        return lax.rem(z + dz + NZ, NZ) * NX + lax.rem(x + dx + NX, NX)

    barrier = pltpu.get_barrier_semaphore()

    def greet(**device):
        pl.semaphore_signal(barrier, inc=1, device_id=device, device_id_type=MESH)

    for o in (1, 2, 3):
        for p in range(2):
            greet(tp=tp_at(o, p))
    greet(tp=sibling)
    for j in range(1, NZ):
        greet(sp=sp_at(j, 0))
    for k in range(1, NX):
        greet(sp=sp_at(0, k))
    greet(sp=lax.rem(place + sp - 1, sp))

    def columns(owner):
        return pl.ds(pl.multiple_of(owner * part, part), part)

    def at(t):
        return pl.ds(pl.multiple_of(t * BLOCK, BLOCK), BLOCK)

    def load(i, src, dst):
        return pltpu.make_async_copy(src, dst, l_sem.at[i])

    loads = {"tok": load(0, tok_hbm, full.at[:, columns(me)]), "oc": load(1, oc_hbm, wc.at[0, :BLOCK, :])}
    for i, src in enumerate((wq_hbm, wk_hbm, wv_hbm, wdg_hbm, wgv_hbm, wgg_hbm, wcg_hbm)):
        loads[i] = load(2 + i, src, w_all.at[:, i * width : (i + 1) * width])
    loads["wb"] = load(9, wb_hbm, wb_s)
    loads["wdec"] = load(10, wdec_hbm, wdec_s)
    loads["rate"] = load(11, rate_hbm, rate_s)
    loads["gain"] = load(12, gain_hbm, gain_s)
    loads["taps"] = load(13, taps_hbm, taps_s)
    loads["lng"] = load(14, lng_hbm, lng_s)
    loads["lns"] = load(15, lns_hbm, lns_s)
    loads["od"] = load(16, od_hbm, wd.at[0, :BLOCK, :])
    for copy in loads.values():
        copy.start()

    def remote(src, dst, send, recv, **device):
        return pltpu.make_async_remote_copy(
            src_ref=src, dst_ref=dst, send_sem=send, recv_sem=recv,
            device_id=device, device_id_type=MESH,
        )

    def to_right(r):
        block = full.at[at(r), columns(me)]
        return remote(block, block, r_send.at[r], r_recv.at[r], tp=tp_at(1))

    def to_left(r):
        block = full.at[at(r), columns(me)]
        return remote(block, block, l_send.at[r], l_recv.at[r], tp=tp_at(-1))

    def half(r, i):
        return pl.ds(pl.multiple_of(r * BLOCK + i * (BLOCK // 2), BLOCK // 2), BLOCK // 2)

    def on_right(r):
        block = full.at[half(r, 0), columns(tp_at(-1))]
        return remote(block, block, fr_send.at[r], fr_recv.at[r], tp=tp_at(1))

    def on_left(r):
        block = full.at[half(r, 1), columns(tp_at(1))]
        return remote(block, block, fl_send.at[r], fl_recv.at[r], tp=tp_at(-1))

    def beside(o, r):
        block = full.at[at(r), columns(tp_at(o))]
        return remote(block, block, b_send.at[o, r], b_recv.at[o, r], tp=sibling)

    zrows = BLOCK // NZ
    xcols = wc.shape[2] // NX

    def wpiece(i):
        return (
            pl.ds(pl.multiple_of(lax.rem(z - i + NZ, NZ) * zrows, zrows), zrows),
            pl.ds(pl.multiple_of(x * xcols, xcols), xcols),
        )

    def w_first(o):
        a, b = wpiece(0)
        return remote(
            wc.at[0, a, b], wc.at[NY - o, a, b], w1_send.at[o - 1], w1_recv.at[o - 1], tp=tp_at(o)
        )

    def w_second(j):
        a, b = wpiece(0)
        block = wc.at[pl.ds(1, NY - 1), a, b]
        return remote(block, block, w2_send.at[j - 1], w2_recv.at[j - 1], sp=sp_at(j, 0))

    def w_third(i, k):
        a, b = wpiece(i)
        block = wc.at[pl.ds(1, NY - 1), a, b]
        return remote(block, block, w3_send.at[i, k - 1], w3_recv.at[i, k - 1], sp=sp_at(0, k))

    def w_beside():
        return remote(
            wc.at[:, pl.ds(0, BLOCK), :], wc.at[:, pl.ds(BLOCK, BLOCK), :],
            wb_send.at[NY], wb_recv.at[NY], tp=sibling,
        )

    def d_beside(d):
        return remote(
            wd.at[d, pl.ds(0, BLOCK), :], wd.at[d, pl.ds(BLOCK, BLOCK), :],
            wb_send.at[d], wb_recv.at[d], tp=sibling,
        )

    hb = BLOCK // 2

    def d_right(i):
        return remote(
            wd.at[0, pl.ds(i * hb, hb), :], wd.at[3, pl.ds(i * hb, hb), :],
            wd_send.at[i], wd_recv.at[i], tp=tp_at(1),
        )

    def d_left(i):
        return remote(
            wd.at[0, pl.ds((1 - i) * hb, hb), :], wd.at[1, pl.ds((1 - i) * hb, hb), :],
            wd_send.at[2 + i], wd_recv.at[2 + i], tp=tp_at(-1),
        )

    def d_on_right():
        return remote(
            wd.at[3, pl.ds(0, hb), :], wd.at[2, pl.ds(0, hb), :],
            wd_send.at[4], wd_recv.at[4], tp=tp_at(1),
        )

    def d_on_left():
        return remote(
            wd.at[1, pl.ds(hb, hb), :], wd.at[2, pl.ds(hb, hb), :],
            wd_send.at[5], wd_recv.at[5], tp=tp_at(-1),
        )

    loads["tok"].wait()
    loads["oc"].wait()
    pl.semaphore_wait(barrier, 7 + NZ - 1 + NX - 1 + 1)
    for o in (2, 1, 3):
        w_first(o).start()
    for r in range(AHEAD):
        to_right(r).start()
        to_left(r).start()

    def own_beside(r, carry):
        beside(0, r).start()
        return carry

    lax.fori_loop(0, chunks, own_beside, 0)

    loads["wb"].wait()
    loads["wdec"].wait()
    loads["rate"].wait()
    heads = wb_s.shape[0]
    pick = lax.broadcasted_iota(jnp.int32, wb_s.shape, 0) == me
    beta_row = jnp.sum(jnp.where(pick, wb_s[...].astype(F32), 0.0), axis=0, keepdims=True)
    decay_row = jnp.sum(jnp.where(pick, wdec_s[...].astype(F32), 0.0), axis=0, keepdims=True)
    sub_id = lax.broadcasted_iota(jnp.int32, (BLOCK, BLOCK), 0)
    for b in range(2 * NY * part // BLOCK):
        cut = slice(b * BLOCK, (b + 1) * BLOCK)
        tall = jnp.where(sub_id == 0, beta_row[:, cut], jnp.where(sub_id == 1, decay_row[:, cut], 0.0))
        w_all[cut, 7 * width : 8 * width] = tall.T.astype(BF16)
    lane8 = lax.broadcasted_iota(jnp.int32, (1, heads), 1)
    rate = jnp.exp(
        jnp.sum(jnp.where(lane8 == me, rate_s[...], 0.0), axis=1, keepdims=True)
    )
    for i in range(7):
        loads[i].wait()
    loads["taps"].wait()
    tapf_s[:kernel, :] = taps_s[...].astype(F32)

    def arrive(r):
        to_right(r).wait_recv()
        to_left(r).wait_recv()
        on_right(r).start()
        on_left(r).start()
        beside(3, r).start()
        beside(1, r).start()

        @pl.when(r + AHEAD < chunks)
        def _():
            to_right(r + AHEAD).start()
            to_left(r + AHEAD).start()

    def arrive_far(r):
        on_right(r).wait_recv()
        on_left(r).wait_recv()
        beside(2, r).start()

    def w_pass(r):
        w_second(r).wait_recv()
        for k in (2, 1, 3):
            w_third(r, k).start()

    def chunk(r):
        for o in range(NY):
            beside(o, r).wait_recv()
        here = at(r)
        squares = jnp.zeros((BLOCK, 1), F32)
        for b in range(2 * NY):
            piece = full[here, b * part : (b + 1) * part].astype(F32)
            squares = squares + jnp.sum(piece * piece, axis=1, keepdims=True)
        inv_rms = lax.rsqrt(squares / (part * 2 * NY) + TINY_NORM)
        for j in range(4):
            summed = jnp.dot(
                full[here, :], w_all[:, j * 256 : (j + 1) * 256], preferred_element_type=F32
            )
            summed = summed * inv_rms
            proj[2 * j, here, :] = summed[:, :width].astype(BF16)
            if j < 3:
                proj[2 * j + 1, here, :] = summed[:, width:].astype(BF16)
            else:
                raw = summed[:, width:]
                lane = lax.broadcasted_iota(jnp.int32, raw.shape, 1)
                softplus = jnp.maximum(raw, 0.0) + jnp.log1p(jnp.exp(-jnp.abs(raw)))
                gates_ref[here, :] = jnp.where(
                    lane == 0, jax.nn.sigmoid(raw), jnp.where(lane == 1, -rate * softplus, 0.0)
                )

    row_id = lax.broadcasted_iota(jnp.int32, (BLOCK, BLOCK), 0)
    col_id = lax.broadcasted_iota(jnp.int32, (BLOCK, BLOCK), 1)
    causal = row_id >= col_id
    strict = row_id > col_id
    differ = row_id ^ col_id
    eye = jnp.where(row_id == col_id, 1.0, 0.0)
    tril = jnp.where(causal, 1.0, 0.0)
    ident = jnp.concatenate([eye, jnp.zeros((width, width), F32)], axis=1)

    def prepare(c):
        here = slice(c * BLOCK, (c + 1) * BLOCK)
        gates = gates_ref[here, :]
        sums = jnp.dot(tril, gates, precision=HIGHEST, preferred_element_type=F32)
        q, k = proj[0, here, :], proj[1, here, :]
        v = proj[2, here, :].astype(F32)
        kf, qf = k.astype(F32), q.astype(F32)
        ik = lax.rsqrt(jnp.sum(kf * kf, axis=-1, keepdims=True) + TINY_NORM)
        iq = lax.rsqrt(jnp.sum(qf * qf, axis=-1, keepdims=True) + TINY_NORM)
        iq = iq * width ** (-0.5)
        beta = gates[:, 0:1]
        log_sum = sums[:, 1:2]
        log_full = jnp.broadcast_to(log_sum, (BLOCK, BLOCK))
        spread = log_full - log_full.T
        damp = jnp.where(causal, jnp.exp(jnp.where(causal, spread, 0.0)), 0.0)
        damp = damp * jnp.broadcast_to(ik, (BLOCK, BLOCK)).T
        lower = jnp.where(strict, nt(k, k) * damp * (beta * ik), 0.0)
        score_s[here, :] = (nt(q, k) * damp * iq).astype(BF16)
        grow = jnp.exp(log_sum)
        right = jnp.concatenate([v * beta, kf * (beta * ik * grow)], axis=1)
        tail = log_full[BLOCK - 1 : BLOCK, :]
        weighted = kf * (ik * jnp.exp(tail[:, :1] - log_sum))
        wt_s[c] = weighted.T.astype(BF16)
        tail_s[c] = jnp.broadcast_to(jnp.exp(tail), (8, BLOCK))
        lhs_s[c, BLOCK:, :] = (qf * (iq * grow)).astype(BF16)
        return [c, lower, right, eye - jnp.where(differ == 1, lower, 0.0)]

    def advance(c, carry):
        both = mm(lhs_s[c], state_ref[...])
        first = both[:BLOCK]
        fresh = jnp.concatenate(
            [-first[:, :width], corr_s[at(c), :] - first[:, width:]], axis=1
        ).astype(BF16)
        decay = tail_s[c][:1, :]
        decay = jnp.concatenate([decay, decay], axis=1)
        state_ref[...] = state_ref[...] * decay + mm(wt_s[c], fresh)
        out = both[BLOCK:] + mm(score_s[at(c), :], fresh)
        outa_s[at(c), :] = out[:, :width].astype(BF16)
        outb_s[at(c), :] = out[:, width:]
        return carry

    def delta_group(first, count, pauses=()):
        chains = [prepare(first + i) for i in range(count)]
        size = 2
        while size < BLOCK:
            if size in pauses:
                yield
            level = (differ >= size) & (differ < 2 * size)
            moved = [mm(jnp.where(level, ch[1], 0.0), ch[3]) for ch in chains]
            for ch, part_ in zip(chains, moved):
                ch[3] = ch[3] - mm(ch[3], part_)
            size *= 2
        for c, lower, right, inverse in chains:
            solved = mm(inverse, right)
            corr_s[c * BLOCK : (c + 1) * BLOCK, :] = solved[:, :width]
            lhs_s[c, :BLOCK, :] = solved[:, width:].astype(BF16)
        lax.fori_loop(first, first + count, advance, 0)

    state_ref[...] = ident
    for o in (1, 2, 3):
        w_first(o).wait_recv()
    for j in range(1, NZ):
        w_second(j).start()
    for k in (2, 1, 3):
        w_third(0, k).start()
    arrive(0)
    arrive(1)
    arrive_far(0)
    w_pass(1)

    def steady(r, carry):
        arrive(r)
        arrive_far(r - 1)
        chunk(r - 2)
        w_pass(r)
        return carry

    lax.fori_loop(2, 6, steady, 0)
    early = delta_group(0, 4, (8, 64))
    arrive(6)
    arrive_far(5)
    next(early)
    chunk(4)
    w_pass(6)
    arrive(7)
    loads["od"].wait()
    for i in range(2):
        d_right(i).start()
        d_left(i).start()
    arrive_far(6)
    next(early)
    chunk(5)
    w_pass(7)
    arrive_far(7)
    list(early)
    chunk(6)
    chunk(7)

    def unit(t):
        value = proj[4, at(t), :].astype(F32)
        units = (value * jax.nn.sigmoid(proj[5, at(t), :].astype(F32))).astype(BF16)
        padded[pl.ds(pl.multiple_of(t * BLOCK + halo, halo), BLOCK), :] = units.astype(F32)
        return units

    units = unit(chunks - 1)
    halo_out[...] = units[BLOCK - halo :, :]
    halo_copy = remote(
        halo_out, halo_in, h_send.at[0], h_recv.at[0], sp=lax.rem(place + 1, sp)
    )

    @pl.when(place + 1 < sp)
    def _():
        halo_copy.start()

    list(delta_group(4, 4))

    xin[0] = state_ref[...].astype(BF16)

    def x_copy(k):
        return remote(xin.at[0], xin.at[k], x_send.at[k - 1], x_recv.at[k - 1], sp=sp_at(0, k))

    for k in (2, 1, 3):
        x_copy(k).start()

    def unit_loop(t, carry):
        unit(t)
        return carry

    for i in range(NZ):
        for k in range(1, NX):
            w_third(i, k).wait_recv()
    w_beside().start()
    lax.fori_loop(0, chunks - 1, unit_loop, 0)

    def conv(t, carry):
        total = jnp.zeros((BLOCK, width), F32)
        for j in range(kernel):
            start = t * BLOCK + (halo - kernel + 1 + j)
            total = total + padded[pl.ds(start, BLOCK), :] * tapf_s[j : j + 1, :]
        filtered[at(t), :] = total
        first = jnp.sum(total, axis=1, keepdims=True)
        second = jnp.sum(total * total, axis=1, keepdims=True)
        turned = jnp.where(col_id == 0, first, jnp.where(col_id == 1, second, 0.0)).T
        sums_out[pl.ds(t, 1), :] = turned[0:1, :]
        sums_out[pl.ds(t + 8, 1), :] = turned[1:2, :]
        return carry

    lax.fori_loop(1, chunks, conv, 0)
    for i in range(2):
        d_right(i).wait_recv()
        d_left(i).wait_recv()
    d_on_right().start()
    d_on_left().start()
    for d in (0, 1, 3):
        d_beside(d).start()

    for k in (1, 2, 3):
        x_copy(k).wait_recv()

    def piece(i):
        return xin[lax.rem(x - i + NX, NX)]

    p0, p1, p2, p3 = (piece(i) for i in range(NX))
    w2 = compose(p1, p0)
    pair = compose(p3, p2)
    group = compose(pair, w2)
    w3 = compose(p2, w2)
    inner = jnp.where(
        x == 0, ident, jnp.where(x == 1, p0.astype(F32), jnp.where(x == 2, w2, w3))
    ).astype(BF16)
    zs[0] = group.astype(BF16)

    def z_copy(i, b):
        cut = pl.ds(b * width, width)
        return remote(
            zs.at[i, :, cut], zr.at[i, :, cut],
            z_send.at[2 * i + b], z_recv.at[2 * i + b], sp=sp_at(i + 1, 0),
        )

    last_copy = remote(zs4, zr4, z_send.at[4], z_recv.at[4], sp=sp_at(4, 0))

    def z_start(i, b):
        @pl.when(z + i + 1 < NZ)
        def _():
            z_copy(i, b).start()

    def z_wait(i, b):
        @pl.when(z >= i + 1)
        def _():
            z_copy(i, b).wait_recv()

    z_start(0, 1)
    z_start(0, 0)

    for i in range(2):

        @pl.when(z < i + 1)
        def _(i=i):
            zr[i] = ident.astype(BF16)

    @pl.when(z < 4)
    def _():
        zr4[...] = jnp.zeros(zr4.shape, BF16)

    @pl.when(place >= 1)
    def _():
        halo_copy.wait_recv()

    @pl.when(place < 1)
    def _():
        halo_in[...] = jnp.zeros(halo_in.shape, BF16)

    padded[:halo, :] = halo_in[...].astype(F32)
    conv(0, 0)

    def ln_copy(o, p):
        i = 2 * o + p - 1
        return remote(
            sums_out, sums_in.at[i], ln_send.at[i], ln_recv.at[i], tp=tp_at(o, p)
        )

    others = [(2, 0), (2, 1), (1, 0), (1, 1), (3, 0), (3, 1), (0, 1)]
    for o, p in others:
        ln_copy(o, p).start()
    def drain(r, carry):
        to_right(r).wait_send()
        to_left(r).wait_send()
        on_right(r).wait_send()
        on_left(r).wait_send()
        for o in range(NY):
            beside(o, r).wait_send()
        for k in range(1, NX):
            w_third(r, k).wait_send()
        return carry

    lax.fori_loop(0, chunks, drain, 0)
    for o in (1, 2, 3):
        w_first(o).wait_send()
    for j in range(1, NZ):
        w_second(j).wait_send()
    for k in (1, 2, 3):
        x_copy(k).wait_send()

    def left(i):
        return zs[i][:, :width]

    z_wait(0, 1)
    zs[1, :, width:] = (
        mm(left(0), zr[0, :, width:]) + zs[0, :, width:].astype(F32)
    ).astype(BF16)
    z_start(1, 1)
    z_wait(0, 0)
    e1 = zr[0]
    zs[1, :, :width] = mm(left(0), e1[:, :width]).astype(BF16)
    z_start(1, 0)

    for o, p in others:
        ln_copy(o, p).wait_recv()
    loads["lng"].wait()
    loads["lns"].wait()
    loads["gain"].wait()
    sums = sums_out[...]
    for i in range(7):
        sums = sums + sums_in[i]
    sums = jnp.concatenate([sums, jnp.zeros((BLOCK - 16, BLOCK), F32)], axis=0).T
    channels = width * 2 * NY
    center_all = sums[:, 0:8] / channels
    variance = jnp.maximum(sums[:, 8:16] / channels - center_all * center_all, 0.0)
    scale_all = lax.rsqrt(variance + TINY_VAR)
    for t in range(chunks):
        here = slice(t * BLOCK, (t + 1) * BLOCK)
        normed = (filtered[here, :] - center_all[:, t : t + 1]) * scale_all[:, t : t + 1]
        normed = normed * lng_s[...] + lns_s[...]
        gate = proj[6, here, :].astype(F32)
        cm_s[here, :] = (jax.nn.silu(normed) * jax.nn.silu(gate)).astype(BF16)

    def c_copy(o, p):
        i = 2 * o + p - 1
        return remote(
            cm_s.at[at(tp_at(o, p)), :],
            in_c.at[(NY - o) % NY, :, pl.ds(p * width, width)],
            c_send.at[i], c_recv.at[i], tp=tp_at(o, p),
        )

    for o, p in others:
        c_copy(o, p).start()
    in_c[0, :, :width] = cm_s[at(me), :]
    d_on_right().wait_recv()
    d_on_left().wait_recv()
    d_beside(2).start()
    z_wait(1, 1)
    zs4[...] = (mm(left(1), zr[1, :, width:]) + zs[1, :, width:].astype(F32)).astype(BF16)

    @pl.when(z + 4 < NZ)
    def _():
        last_copy.start()

    z_wait(1, 0)
    e3 = compose(e1, zr[1])
    reach = compose(inner, e3)

    for t in range(chunks):
        here = slice(t * BLOCK, (t + 1) * BLOCK)
        gate_s[here, :] = gain_s[...] * jax.nn.silu(proj[3, here, :].astype(F32))

    w_beside().wait_recv()
    for o, p in others:
        c_copy(o, p).wait_recv()
    step = 512
    cuts = out_ref.shape[1] // step

    def out_copy(n):
        cut = pl.ds(n * step, step)
        return pltpu.make_async_copy(out_ref.at[:, cut], out_hbm.at[:, cut], o_sem.at[n])

    for n in range(cuts):
        cut = slice(n * step, (n + 1) * step)
        total = jnp.zeros((BLOCK, step), F32)
        for d in range(NY):
            total = total + jnp.dot(in_c[d], wc[d, :, cut], preferred_element_type=F32)
        acc[:, cut] = total

    @pl.when(z >= 4)
    def _():
        last_copy.wait_recv()

    carried = (mm(reach[:, :width], zr4[...]) + reach[:, width:]).astype(BF16)

    def d_copy(o, p):
        i = 2 * o + p - 1
        return remote(
            dsend.at[i], in_d.at[(NY - o) % NY, :, pl.ds(p * width, width)],
            d_send.at[i], d_recv.at[i], tp=tp_at(o, p),
        )

    for batch in (others[:2], others[2:6], [(0, 1), (0, 0)]):
        places = [at(tp_at(o, p)) for o, p in batch]
        results = [outb_s[pos, :] + mm(outa_s[pos, :], carried) for pos in places]
        scales = [
            lax.rsqrt(jnp.mean(res * res, axis=-1, keepdims=True) + TINY_NORM) for res in results
        ]
        mixed = [
            (res * sc * gate_s[pos, :]).astype(BF16)
            for res, sc, pos in zip(results, scales, places)
        ]
        for (o, p), value in zip(batch, mixed):
            if o == 0 and p == 0:
                in_d[0, :, :width] = value
            else:
                dsend[2 * o + p - 1] = value
        for o, p in batch:
            if o or p:
                d_copy(o, p).start()

    for d in range(NY):
        d_beside(d).wait_recv()
    for group_at in ((0,), (3, 1), (2,)):
        for d in group_at:
            o = (NY - d) % NY
            for p in range(2):
                if o or p:
                    d_copy(o, p).wait_recv()
        for n in range(cuts):
            cut = slice(n * step, (n + 1) * step)
            total = acc[:, cut]
            for d in group_at:
                total = total + jnp.dot(in_d[d], wd[d, :, cut], preferred_element_type=F32)
            if group_at == (2,):
                out_ref[:, cut] = total.astype(BF16)
                out_copy(n).start()
            else:
                acc[:, cut] = total

    for i in range(2):
        d_right(i).wait_send()
        d_left(i).wait_send()
    d_on_right().wait_send()
    d_on_left().wait_send()
    w_beside().wait_send()
    for d in range(NY):
        d_beside(d).wait_send()

    @pl.when(place + 1 < sp)
    def _():
        halo_copy.wait_send()

    for i in range(2):

        @pl.when(z + i + 1 < NZ)
        def _(i=i):
            z_copy(i, 0).wait_send()
            z_copy(i, 1).wait_send()

    @pl.when(z + 4 < NZ)
    def _():
        last_copy.wait_send()

    for o, p in others:
        ln_copy(o, p).wait_send()
        c_copy(o, p).wait_send()
        d_copy(o, p).wait_send()
    for n in range(cuts):
        out_copy(n).wait()


def local(
    tokens, w_query, w_key, w_value, w_delta_gate, w_glu_value, w_glu_gate, w_conv_gate,
    w_beta, w_decay, decay_log, head_gain, conv_taps, ln_gain, ln_shift, out_delta, out_conv,
):
    rows, part = tokens.shape
    depth, width = w_query.shape
    wide = out_delta.shape[1]
    heads = w_beta.shape[1]
    chunks = rows // BLOCK
    kernel = conv_taps.shape[0]
    halo = (kernel - 1 + 31) // 32 * 32
    hbm = pl.BlockSpec(memory_space=pltpu.HBM)
    dma = pltpu.SemaphoreType.DMA
    vm = pltpu.VMEM
    return pl.pallas_call(
        layer_kernel,
        out_shape=jax.ShapeDtypeStruct((BLOCK, wide), BF16),
        in_specs=[hbm] * 17,
        out_specs=hbm,
        scratch_shapes=[
            vm((BLOCK, wide), BF16),
            vm((rows, depth), BF16),
            vm((depth, 8 * width), BF16),
            vm((7, rows, width), BF16),
            vm((rows, width), F32),
            vm((heads, depth), BF16),
            vm((heads, depth), BF16),
            vm((1, heads), F32),
            vm((1, width), F32),
            vm((kernel, width), BF16),
            vm((32, width), F32),
            vm((1, width), F32),
            vm((1, width), F32),
            vm((NY, 2 * BLOCK, wide), BF16),
            vm((NY, 2 * BLOCK, wide), BF16),
            vm((chunks, 2 * BLOCK, width), BF16),
            vm((rows, width), F32),
            vm((rows, BLOCK), BF16),
            vm((chunks, width, BLOCK), BF16),
            vm((chunks, 8, BLOCK), F32),
            vm((width, 2 * width), F32),
            vm((rows, width), BF16),
            vm((rows, width), F32),
            vm((NX, width, 2 * width), BF16),
            vm((2, width, 2 * width), BF16),
            vm((2, width, 2 * width), BF16),
            vm((width, width), BF16),
            vm((width, width), BF16),
            vm((halo + rows, width), F32),
            vm((rows, width), F32),
            vm((halo, width), BF16),
            vm((halo, width), BF16),
            vm((16, BLOCK), F32),
            vm((7, 16, BLOCK), F32),
            vm((rows, width), BF16),
            vm((7, BLOCK, width), BF16),
            vm((NY, BLOCK, 2 * width), BF16),
            vm((NY, BLOCK, 2 * width), BF16),
            vm((BLOCK, wide), F32),
            vm((rows, width), F32),
            dma((17,)),
            dma((chunks,)), dma((chunks,)), dma((chunks,)), dma((chunks,)),
            dma((chunks,)), dma((chunks,)), dma((chunks,)), dma((chunks,)),
            dma((NY, chunks)), dma((NY, chunks)),
            dma((NY - 1,)), dma((NY - 1,)),
            dma((NZ - 1,)), dma((NZ - 1,)),
            dma((NZ, NX - 1)), dma((NZ, NX - 1)),
            dma((NY + 1,)), dma((NY + 1,)),
            dma((6,)), dma((6,)),
            dma((NX - 1,)), dma((NX - 1,)),
            dma((5,)), dma((5,)),
            dma((1,)), dma((1,)),
            dma((7,)), dma((7,)),
            dma((7,)), dma((7,)),
            dma((7,)), dma((7,)),
            dma((4,)),
        ],
        compiler_params=pltpu.CompilerParams(
            collective_id=0, has_side_effects=True, vmem_limit_bytes=60 * 1024 * 1024
        ),
        cost_estimate=pl.CostEstimate(
            flops=10_000_000_000, bytes_accessed=20_000_000, transcendentals=0
        ),
        name="layer",
    )(
        tokens, w_query, w_key, w_value, w_delta_gate, w_glu_value, w_glu_gate, w_conv_gate,
        w_beta.T, w_decay.T, decay_log[None, :], head_gain[None, :], conv_taps,
        ln_gain[None, :], ln_shift[None, :], out_delta, out_conv,
    )


def solution(mesh):
    return jax.shard_map(
        local,
        mesh=mesh,
        in_specs=(
            P("sp", "tp"), P(None, "tp"), P(None, "tp"), P(None, "tp"), P(None, "tp"),
            P(None, "tp"), P(None, "tp"), P(None, "tp"), P(), P(), P(), P(), P(None, "tp"),
            P("tp"), P("tp"), P("tp", None), P("tp", None),
        ),
        out_specs=P(("sp", "tp"), None),
        check_vma=False,
    )
```

```python
import jax
import jax.numpy as jnp
from jax import lax
from jax.experimental import pallas as pl
from jax.experimental.pallas import tpu as pltpu
from jax.sharding import PartitionSpec as P

BLOCK = 128
AHEAD = 3
TINY_NORM = 1e-06
TINY_VAR = 1e-05
HIGHEST = lax.Precision.HIGHEST
MESH = pl.DeviceIdType.MESH
F32 = jnp.float32
BF16 = jnp.bfloat16
NX = 4
NZ = 8
NY = 4


def nt(a, b):
    return lax.dot_general(a, b, (((1,), (1,)), ((), ())), preferred_element_type=F32)


def mm(a, b):
    return jnp.dot(a.astype(BF16), b.astype(BF16), preferred_element_type=F32)


def compose(later, earlier):
    width = later.shape[0]
    moved = mm(later[:, :width], earlier)
    return jnp.concatenate(
        [moved[:, :width], moved[:, width:] + later[:, width:].astype(F32)], axis=1
    )


def layer_kernel(
    tok_hbm, wq_hbm, wk_hbm, wv_hbm, wdg_hbm, wgv_hbm, wgg_hbm, wcg_hbm, wb_hbm, wdec_hbm,
    rate_hbm, gain_hbm, taps_hbm, lng_hbm, lns_hbm, od_hbm, oc_hbm,
    out_hbm,
    out_ref, full, w_all, proj, gates_ref, wb_s, wdec_s, rate_s, gain_s, taps_s, tapf_s, lng_s, lns_s,
    wd, wc, lhs_s, corr_s, score_s, wt_s, tail_s, state_ref, outa_s, outb_s,
    xin, zs, zr, zs4, zr4, padded, filtered, halo_out, halo_in, sums_out, sums_in,
    cm_s, dsend, in_d, in_c, acc, gate_s,
    l_sem, sent, a_recv, f_recv, b_recv, w2_recv, got, z_send, z_recv,
):
    rows, part = tok_hbm.shape
    chunks = rows // BLOCK
    width = gain_hbm.shape[1]
    halo = halo_in.shape[0]
    kernel = taps_hbm.shape[0]
    sp, place = NX * NZ, lax.axis_index("sp")
    me = lax.axis_index("tp")
    core, y = lax.rem(me, 2), me // 2
    x, z = lax.rem(place, NX), place // NX
    sibling = me + 1 - 2 * core

    def tp_at(o, p=0):
        side = core + p * (1 - 2 * core)
        return lax.rem(y + o + NY, NY) * 2 + side

    def sp_at(dz, dx):
        return lax.rem(z + dz + NZ, NZ) * NX + lax.rem(x + dx + NX, NX)

    barrier = pltpu.get_barrier_semaphore()

    def greet(**device):
        pl.semaphore_signal(barrier, inc=1, device_id=device, device_id_type=MESH)

    for o in (1, 2, 3):
        for p in range(2):
            greet(tp=tp_at(o, p))
    greet(tp=sibling)
    for j in range(1, NZ):
        greet(sp=sp_at(j, 0))
    for k in range(1, NX):
        greet(sp=sp_at(0, k))
    greet(sp=lax.rem(place + sp - 1, sp))

    def columns(owner):
        return pl.ds(pl.multiple_of(owner * part, part), part)

    def at(t):
        return pl.ds(pl.multiple_of(t * BLOCK, BLOCK), BLOCK)

    def load(i, src, dst):
        return pltpu.make_async_copy(src, dst, l_sem.at[i])

    loads = {"tok": load(0, tok_hbm, full.at[:, columns(me)]), "oc": load(1, oc_hbm, wc.at[0, :BLOCK, :])}
    for i, src in enumerate((wq_hbm, wk_hbm, wv_hbm, wdg_hbm, wgv_hbm, wgg_hbm, wcg_hbm)):
        loads[i] = load(2, src, w_all.at[:, i * width : (i + 1) * width])
    loads["wb"] = load(3, wb_hbm, wb_s)
    loads["wdec"] = load(4, wdec_hbm, wdec_s)
    loads["rate"] = load(5, rate_hbm, rate_s)
    loads["gain"] = load(6, gain_hbm, gain_s)
    loads["taps"] = load(7, taps_hbm, taps_s)
    loads["lng"] = load(8, lng_hbm, lng_s)
    loads["lns"] = load(9, lns_hbm, lns_s)
    loads["od"] = load(10, od_hbm, wd.at[0, :BLOCK, :])
    for copy in loads.values():
        copy.start()

    def remote(src, dst, send, recv, **device):
        return pltpu.make_async_remote_copy(
            src_ref=src, dst_ref=dst, send_sem=send, recv_sem=recv,
            device_id=device, device_id_type=MESH,
        )

    def settle(ref, send):
        remote(ref, ref, sent.at[send], got.at[0], tp=sibling).wait_send()

    def landed(ref, recv):
        remote(ref, ref, sent.at[0], recv, tp=sibling).wait_recv()

    def to_right(r):
        block = full.at[at(r), columns(me)]
        return remote(block, block, sent.at[0], a_recv.at[r], tp=tp_at(1))

    def to_left(r):
        block = full.at[at(r), columns(me)]
        return remote(block, block, sent.at[1], a_recv.at[r], tp=tp_at(-1))

    def half(r, i):
        return pl.ds(pl.multiple_of(r * BLOCK + i * (BLOCK // 2), BLOCK // 2), BLOCK // 2)

    def on_right(r):
        block = full.at[half(r, 0), columns(tp_at(-1))]
        return remote(block, block, sent.at[2], f_recv.at[r], tp=tp_at(1))

    def on_left(r):
        block = full.at[half(r, 1), columns(tp_at(1))]
        return remote(block, block, sent.at[3], f_recv.at[r], tp=tp_at(-1))

    def beside(o, r):
        block = full.at[at(r), columns(tp_at(o))]
        return remote(block, block, sent.at[4], b_recv.at[r], tp=sibling)

    zrows = BLOCK // NZ
    xcols = wc.shape[2] // NX

    def wpiece(i):
        return (
            pl.ds(pl.multiple_of(lax.rem(z - i + NZ, NZ) * zrows, zrows), zrows),
            pl.ds(pl.multiple_of(x * xcols, xcols), xcols),
        )

    def w_first(o):
        a, b = wpiece(0)
        return remote(
            wc.at[0, a, b], wc.at[NY - o, a, b], sent.at[5], got.at[1], tp=tp_at(o)
        )

    def w_second(j):
        a, b = wpiece(0)
        block = wc.at[pl.ds(1, NY - 1), a, b]
        return remote(block, block, sent.at[6], w2_recv.at[j - 1], sp=sp_at(j, 0))

    def w_third(i, k):
        a, b = wpiece(i)
        block = wc.at[pl.ds(1, NY - 1), a, b]
        return remote(block, block, sent.at[7], got.at[2], sp=sp_at(0, k))

    def w_beside():
        return remote(
            wc.at[:, pl.ds(0, BLOCK), :], wc.at[:, pl.ds(BLOCK, BLOCK), :],
            sent.at[8], got.at[3], tp=sibling,
        )

    def d_beside(d):
        return remote(
            wd.at[d, pl.ds(0, BLOCK), :], wd.at[d, pl.ds(BLOCK, BLOCK), :],
            sent.at[9], got.at[4], tp=sibling,
        )

    hb = BLOCK // 2

    def d_right(i):
        return remote(
            wd.at[0, pl.ds(i * hb, hb), :], wd.at[3, pl.ds(i * hb, hb), :],
            sent.at[10], got.at[5], tp=tp_at(1),
        )

    def d_left(i):
        return remote(
            wd.at[0, pl.ds((1 - i) * hb, hb), :], wd.at[1, pl.ds((1 - i) * hb, hb), :],
            sent.at[10], got.at[5], tp=tp_at(-1),
        )

    def d_on_right():
        return remote(
            wd.at[3, pl.ds(0, hb), :], wd.at[2, pl.ds(0, hb), :],
            sent.at[11], got.at[6], tp=tp_at(1),
        )

    def d_on_left():
        return remote(
            wd.at[1, pl.ds(hb, hb), :], wd.at[2, pl.ds(hb, hb), :],
            sent.at[11], got.at[6], tp=tp_at(-1),
        )

    loads["tok"].wait()
    loads["oc"].wait()
    pl.semaphore_wait(barrier, 7 + NZ - 1 + NX - 1 + 1)
    for o in (2, 1, 3):
        w_first(o).start()
    for r in range(AHEAD):
        to_right(r).start()
        to_left(r).start()

    def own_beside(r, carry):
        beside(0, r).start()
        return carry

    lax.fori_loop(0, chunks, own_beside, 0)

    loads["wb"].wait()
    loads["wdec"].wait()
    loads["rate"].wait()
    heads = wb_s.shape[0]
    pick = lax.broadcasted_iota(jnp.int32, wb_s.shape, 0) == me
    beta_row = jnp.sum(jnp.where(pick, wb_s[...].astype(F32), 0.0), axis=0, keepdims=True)
    decay_row = jnp.sum(jnp.where(pick, wdec_s[...].astype(F32), 0.0), axis=0, keepdims=True)
    sub_id = lax.broadcasted_iota(jnp.int32, (BLOCK, BLOCK), 0)
    for b in range(2 * NY * part // BLOCK):
        cut = slice(b * BLOCK, (b + 1) * BLOCK)
        tall = jnp.where(sub_id == 0, beta_row[:, cut], jnp.where(sub_id == 1, decay_row[:, cut], 0.0))
        w_all[cut, 7 * width : 8 * width] = tall.T.astype(BF16)
    lane8 = lax.broadcasted_iota(jnp.int32, (1, heads), 1)
    rate = jnp.exp(
        jnp.sum(jnp.where(lane8 == me, rate_s[...], 0.0), axis=1, keepdims=True)
    )
    load(2, w_all.at[:, : 7 * width], w_all.at[:, : 7 * width]).wait()
    loads["taps"].wait()
    tapf_s[:kernel, :] = taps_s[...].astype(F32)

    def arrive(r):
        landed(full.at[at(r), pl.ds(0, 2 * part)], a_recv.at[r])
        on_right(r).start()
        on_left(r).start()
        beside(3, r).start()
        beside(1, r).start()

        @pl.when(r + AHEAD < chunks)
        def _():
            to_right(r + AHEAD).start()
            to_left(r + AHEAD).start()

    def arrive_far(r):
        landed(full.at[at(r), pl.ds(0, part)], f_recv.at[r])
        beside(2, r).start()

    def w_pass(r):
        w_second(r).wait_recv()
        for k in (2, 1, 3):
            w_third(r, k).start()

    def chunk(r, count=1):
        for i in range(count):
            landed(full.at[at(r + i), pl.ds(0, NY * part)], b_recv.at[r + i])
        size = count * BLOCK
        here = pl.ds(pl.multiple_of(r * BLOCK, BLOCK), size)
        squares = jnp.zeros((size, 1), F32)
        for b in range(2 * NY):
            piece = full[here, b * part : (b + 1) * part].astype(F32)
            squares = squares + jnp.sum(piece * piece, axis=1, keepdims=True)
        inv_rms = lax.rsqrt(squares / (part * 2 * NY) + TINY_NORM)
        for j in range(4):
            summed = jnp.dot(
                full[here, :], w_all[:, j * 256 : (j + 1) * 256], preferred_element_type=F32
            )
            summed = summed * inv_rms
            proj[2 * j, here, :] = summed[:, :width].astype(BF16)
            if j < 3:
                proj[2 * j + 1, here, :] = summed[:, width:].astype(BF16)
            else:
                raw = summed[:, width:]
                lane = lax.broadcasted_iota(jnp.int32, raw.shape, 1)
                softplus = jnp.maximum(raw, 0.0) + jnp.log1p(jnp.exp(-jnp.abs(raw)))
                gates_ref[here, :] = jnp.where(
                    lane == 0, jax.nn.sigmoid(raw), jnp.where(lane == 1, -rate * softplus, 0.0)
                )

    row_id = lax.broadcasted_iota(jnp.int32, (BLOCK, BLOCK), 0)
    col_id = lax.broadcasted_iota(jnp.int32, (BLOCK, BLOCK), 1)
    causal = row_id >= col_id
    strict = row_id > col_id
    differ = row_id ^ col_id
    eye = jnp.where(row_id == col_id, 1.0, 0.0)
    tril = jnp.where(causal, 1.0, 0.0)
    ident = jnp.concatenate([eye, jnp.zeros((width, width), F32)], axis=1)

    def prepare(c):
        here = slice(c * BLOCK, (c + 1) * BLOCK)
        gates = gates_ref[here, :]
        sums = jnp.dot(tril, gates, precision=HIGHEST, preferred_element_type=F32)
        q, k = proj[0, here, :], proj[1, here, :]
        v = proj[2, here, :].astype(F32)
        kf, qf = k.astype(F32), q.astype(F32)
        ik = lax.rsqrt(jnp.sum(kf * kf, axis=-1, keepdims=True) + TINY_NORM)
        iq = lax.rsqrt(jnp.sum(qf * qf, axis=-1, keepdims=True) + TINY_NORM)
        iq = iq * width ** (-0.5)
        beta = gates[:, 0:1]
        log_sum = sums[:, 1:2]
        log_full = jnp.broadcast_to(log_sum, (BLOCK, BLOCK))
        spread = log_full - log_full.T
        damp = jnp.where(causal, jnp.exp(jnp.where(causal, spread, 0.0)), 0.0)
        damp = damp * jnp.broadcast_to(ik, (BLOCK, BLOCK)).T
        lower = jnp.where(strict, nt(k, k) * damp * (beta * ik), 0.0)
        score_s[here, :] = (nt(q, k) * damp * iq).astype(BF16)
        grow = jnp.exp(log_sum)
        right = jnp.concatenate([v * beta, kf * (beta * ik * grow)], axis=1)
        tail = log_full[BLOCK - 1 : BLOCK, :]
        weighted = kf * (ik * jnp.exp(tail[:, :1] - log_sum))
        wt_s[c] = weighted.T.astype(BF16)
        tail_s[c] = jnp.broadcast_to(jnp.exp(tail), (8, BLOCK))
        lhs_s[c, BLOCK:, :] = (qf * (iq * grow)).astype(BF16)
        return [c, lower, right, eye - jnp.where(differ == 1, lower, 0.0)]

    def advance(c, carry):
        both = mm(lhs_s[c], state_ref[...])
        first = both[:BLOCK]
        fresh = jnp.concatenate(
            [-first[:, :width], corr_s[at(c), :] - first[:, width:]], axis=1
        ).astype(BF16)
        decay = tail_s[c][:1, :]
        decay = jnp.concatenate([decay, decay], axis=1)
        state_ref[...] = state_ref[...] * decay + mm(wt_s[c], fresh)
        out = both[BLOCK:] + mm(score_s[at(c), :], fresh)
        outa_s[at(c), :] = out[:, :width].astype(BF16)
        outb_s[at(c), :] = out[:, width:]
        return carry

    def delta_group(first, count, pauses=()):
        chains = [prepare(first + i) for i in range(count)]
        size = 2
        while size < BLOCK:
            if size in pauses:
                yield
            level = (differ >= size) & (differ < 4 * size)
            steps = [mm(ch[3], jnp.where(level, ch[1], 0.0)) for ch in chains]
            once = [ch[3] - mm(step, ch[3]) for ch, step in zip(chains, steps)]
            twice = [mm(step, step) for step in steps]
            for ch, one, two in zip(chains, once, twice):
                ch[3] = one + mm(two, one)
            size *= 4
        if size in pauses:
            yield
        for c, lower, right, inverse in chains:
            solved = mm(inverse, right)
            corr_s[c * BLOCK : (c + 1) * BLOCK, :] = solved[:, :width]
            lhs_s[c, :BLOCK, :] = solved[:, width:].astype(BF16)
        lax.fori_loop(first, first + count, advance, 0)

    state_ref[...] = ident
    landed(wc.at[0, pl.ds(0, 3 * zrows), pl.ds(0, xcols)], got.at[1])
    for j in range(1, NZ):
        w_second(j).start()
    for k in (2, 1, 3):
        w_third(0, k).start()
    arrive(0)
    arrive(1)
    arrive_far(0)
    w_pass(1)

    def steady(r, carry):
        arrive(r)
        arrive_far(r - 1)
        chunk(r - 2)
        w_pass(r)
        return carry

    lax.fori_loop(2, 6, steady, 0)
    early = delta_group(0, 4, (8, BLOCK))
    arrive(6)
    arrive_far(5)
    next(early)
    w_pass(6)
    arrive(7)
    arrive_far(6)
    next(early)
    chunk(4, 2)
    w_pass(7)
    arrive_far(7)
    loads["od"].wait()
    for i in range(2):
        d_right(i).start()
        d_left(i).start()
    list(early)
    chunk(6, 2)

    def unit(t):
        value = proj[4, at(t), :].astype(F32)
        units = (value * jax.nn.sigmoid(proj[5, at(t), :].astype(F32))).astype(BF16)
        padded[pl.ds(pl.multiple_of(t * BLOCK + halo, halo), BLOCK), :] = units.astype(F32)
        return units

    units = unit(chunks - 1)
    halo_out[...] = units[BLOCK - halo :, :]
    halo_copy = remote(
        halo_out, halo_in, sent.at[13], got.at[8], sp=lax.rem(place + 1, sp)
    )

    @pl.when(place + 1 < sp)
    def _():
        halo_copy.start()

    list(delta_group(4, 4))

    xin[0] = state_ref[...].astype(BF16)

    def x_copy(k):
        return remote(xin.at[0], xin.at[k], sent.at[12], got.at[7], sp=sp_at(0, k))

    for k in (2, 1, 3):
        x_copy(k).start()

    def unit_loop(t, carry):
        unit(t)
        return carry

    landed(wc.at[pl.ds(1, NY - 1), pl.ds(0, 96), :], got.at[2])
    w_beside().start()
    lax.fori_loop(0, chunks - 1, unit_loop, 0)

    def conv(t, carry):
        total = jnp.zeros((BLOCK, width), F32)
        for j in range(kernel):
            start = t * BLOCK + (halo - kernel + 1 + j)
            total = total + padded[pl.ds(start, BLOCK), :] * tapf_s[j : j + 1, :]
        filtered[at(t), :] = total
        first = jnp.sum(total, axis=1, keepdims=True)
        second = jnp.sum(total * total, axis=1, keepdims=True)
        turned = jnp.where(col_id == 0, first, jnp.where(col_id == 1, second, 0.0)).T
        sums_out[pl.ds(t, 1), :] = turned[0:1, :]
        sums_out[pl.ds(t + 8, 1), :] = turned[1:2, :]
        return carry

    lax.fori_loop(1, chunks, conv, 0)

    @pl.when(place >= 1)
    def _():
        halo_copy.wait_recv()

    @pl.when(place < 1)
    def _():
        halo_in[...] = jnp.zeros(halo_in.shape, BF16)

    padded[:halo, :] = halo_in[...].astype(F32)
    conv(0, 0)

    def ln_copy(o, p):
        i = 2 * o + p - 1
        return remote(sums_out, sums_in.at[i], sent.at[14], got.at[9], tp=tp_at(o, p))

    others = [(2, 0), (2, 1), (1, 0), (1, 1), (3, 0), (3, 1), (0, 1)]
    for o, p in others:
        ln_copy(o, p).start()
    landed(wd.at[pl.ds(0, 2), pl.ds(0, BLOCK), :], got.at[5])
    d_on_right().start()
    d_on_left().start()
    for d in (0, 1, 3):
        d_beside(d).start()

    landed(xin.at[pl.ds(1, NX - 1)], got.at[7])

    def piece(i):
        return xin[lax.rem(x - i + NX, NX)]

    p0, p1, p2, p3 = (piece(i) for i in range(NX))
    w2 = compose(p1, p0)
    pair = compose(p3, p2)
    group = compose(pair, w2)
    w3 = compose(p2, w2)
    inner = jnp.where(
        x == 0, ident, jnp.where(x == 1, p0.astype(F32), jnp.where(x == 2, w2, w3))
    ).astype(BF16)
    zs[0] = group.astype(BF16)

    def z_copy(i, b):
        cut = pl.ds(b * width, width)
        return remote(
            zs.at[i, :, cut], zr.at[i, :, cut],
            z_send.at[2 * i + b], z_recv.at[2 * i + b], sp=sp_at(i + 1, 0),
        )

    last_copy = remote(zs4, zr4, z_send.at[4], z_recv.at[4], sp=sp_at(4, 0))

    def z_start(i, b):
        @pl.when(z + i + 1 < NZ)
        def _():
            z_copy(i, b).start()

    def z_wait(i, b):
        @pl.when(z >= i + 1)
        def _():
            z_copy(i, b).wait_recv()

    z_start(0, 1)
    z_start(0, 0)

    for i in range(2):

        @pl.when(z < i + 1)
        def _(i=i):
            zr[i] = ident.astype(BF16)

    @pl.when(z < 4)
    def _():
        zr4[...] = jnp.zeros(zr4.shape, BF16)

    settle(full.at[:, columns(me)], 0)
    settle(full.at[:, columns(me)], 1)
    settle(full.at[pl.ds(0, rows // 2), columns(me)], 2)
    settle(full.at[pl.ds(0, rows // 2), columns(me)], 3)
    settle(full.at[:, pl.ds(0, NY * part)], 4)
    settle(wc.at[0, pl.ds(0, 3 * zrows), pl.ds(0, xcols)], 5)
    settle(wc.at[pl.ds(1, NY - 1), pl.ds(0, 7 * zrows), pl.ds(0, xcols)], 6)
    settle(wc.at[pl.ds(1, NY - 1), pl.ds(0, 96), :], 7)
    settle(xin.at[pl.ds(1, NX - 1)], 12)

    def left(i):
        return zs[i][:, :width]

    z_wait(0, 1)
    zs[1, :, width:] = (
        mm(left(0), zr[0, :, width:]) + zs[0, :, width:].astype(F32)
    ).astype(BF16)
    z_start(1, 1)
    z_wait(0, 0)
    e1 = zr[0]
    zs[1, :, :width] = mm(left(0), e1[:, :width]).astype(BF16)
    z_start(1, 0)

    landed(sums_in, got.at[9])
    loads["lng"].wait()
    loads["lns"].wait()
    loads["gain"].wait()
    sums = sums_out[...]
    for i in range(7):
        sums = sums + sums_in[i]
    sums = jnp.concatenate([sums, jnp.zeros((BLOCK - 16, BLOCK), F32)], axis=0).T
    channels = width * 2 * NY
    center_all = sums[:, 0:8] / channels
    variance = jnp.maximum(sums[:, 8:16] / channels - center_all * center_all, 0.0)
    scale_all = lax.rsqrt(variance + TINY_VAR)
    for t in range(chunks):
        here = slice(t * BLOCK, (t + 1) * BLOCK)
        normed = (filtered[here, :] - center_all[:, t : t + 1]) * scale_all[:, t : t + 1]
        normed = normed * lng_s[...] + lns_s[...]
        gate = proj[6, here, :].astype(F32)
        cm_s[here, :] = (jax.nn.silu(normed) * jax.nn.silu(gate)).astype(BF16)

    def c_copy(o, p):
        i = 2 * o + p - 1
        return remote(
            cm_s.at[at(tp_at(o, p)), :],
            in_c.at[(NY - o) % NY, :, pl.ds(p * width, width)],
            sent.at[15], got.at[10], tp=tp_at(o, p),
        )

    for o, p in others:
        c_copy(o, p).start()
    in_c[0, :, :width] = cm_s[at(me), :]
    landed(wd.at[0, pl.ds(0, BLOCK), :], got.at[6])
    d_beside(2).start()
    z_wait(1, 1)
    zs4[...] = (mm(left(1), zr[1, :, width:]) + zs[1, :, width:].astype(F32)).astype(BF16)

    @pl.when(z + 4 < NZ)
    def _():
        last_copy.start()

    z_wait(1, 0)
    e3 = compose(e1, zr[1])
    reach = compose(inner, e3)

    for t in range(chunks):
        here = slice(t * BLOCK, (t + 1) * BLOCK)
        gate_s[here, :] = gain_s[...] * jax.nn.silu(proj[3, here, :].astype(F32))

    w_beside().wait_recv()
    landed(dsend, got.at[10])
    step = 512
    cuts = out_ref.shape[1] // step

    def out_copy(n):
        cut = pl.ds(n * step, step)
        return pltpu.make_async_copy(out_ref.at[:, cut], out_hbm.at[:, cut], l_sem.at[0])

    for n in range(cuts):
        cut = slice(n * step, (n + 1) * step)
        total = jnp.zeros((BLOCK, step), F32)
        for d in range(NY):
            total = total + jnp.dot(in_c[d], wc[d, :, cut], preferred_element_type=F32)
        acc[:, cut] = total

    @pl.when(z >= 4)
    def _():
        last_copy.wait_recv()

    carried = (mm(reach[:, :width], zr4[...]) + reach[:, width:]).astype(BF16)

    def d_copy(o, p):
        i = 2 * o + p - 1
        return remote(
            dsend.at[i], in_d.at[(NY - o) % NY, :, pl.ds(p * width, width)],
            sent.at[16], got.at[0 if o == 0 else 11 if o == 2 else 12], tp=tp_at(o, p),
        )

    for batch in (others[:2], others[2:6], [(0, 1), (0, 0)]):
        places = [at(tp_at(o, p)) for o, p in batch]
        results = [outb_s[pos, :] + mm(outa_s[pos, :], carried) for pos in places]
        scales = [
            lax.rsqrt(jnp.mean(res * res, axis=-1, keepdims=True) + TINY_NORM) for res in results
        ]
        mixed = [
            (res * sc * gate_s[pos, :]).astype(BF16)
            for res, sc, pos in zip(results, scales, places)
        ]
        for (o, p), value in zip(batch, mixed):
            if o == 0 and p == 0:
                in_d[0, :, :width] = value
            else:
                dsend[2 * o + p - 1] = value
        for o, p in batch:
            if o or p:
                d_copy(o, p).start()

    landed(wd.at[:, pl.ds(0, BLOCK), :], got.at[4])
    for group_at, count, sem in (((0,), 1, 0), ((3, 1), 4, 12), ((2,), 2, 11)):
        landed(dsend.at[pl.ds(0, count)], got.at[sem])
        for n in range(cuts):
            cut = slice(n * step, (n + 1) * step)
            total = acc[:, cut]
            for d in group_at:
                total = total + jnp.dot(in_d[d], wd[d, :, cut], preferred_element_type=F32)
            if group_at == (2,):
                out_ref[:, cut] = total.astype(BF16)
                out_copy(n).start()
            else:
                acc[:, cut] = total

    settle(wc.at[:, pl.ds(0, BLOCK), :], 8)
    settle(wd.at[:, pl.ds(0, BLOCK), :], 9)
    settle(wd.at[pl.ds(0, 2), pl.ds(0, BLOCK), :], 10)
    settle(wd.at[0, pl.ds(0, BLOCK), :], 11)

    @pl.when(place + 1 < sp)
    def _():
        halo_copy.wait_send()

    for i in range(2):

        @pl.when(z + i + 1 < NZ)
        def _(i=i):
            z_copy(i, 0).wait_send()
            z_copy(i, 1).wait_send()

    @pl.when(z + 4 < NZ)
    def _():
        last_copy.wait_send()

    settle(sums_in, 14)
    settle(dsend, 15)
    settle(dsend, 16)
    pltpu.make_async_copy(out_ref, out_hbm, l_sem.at[0]).wait()


def local(
    tokens, w_query, w_key, w_value, w_delta_gate, w_glu_value, w_glu_gate, w_conv_gate,
    w_beta, w_decay, decay_log, head_gain, conv_taps, ln_gain, ln_shift, out_delta, out_conv,
):
    rows, part = tokens.shape
    depth, width = w_query.shape
    wide = out_delta.shape[1]
    heads = w_beta.shape[1]
    chunks = rows // BLOCK
    kernel = conv_taps.shape[0]
    halo = (kernel - 1 + 31) // 32 * 32
    hbm = pl.BlockSpec(memory_space=pltpu.HBM)
    dma = pltpu.SemaphoreType.DMA
    vm = pltpu.VMEM
    return pl.pallas_call(
        layer_kernel,
        out_shape=jax.ShapeDtypeStruct((BLOCK, wide), BF16),
        in_specs=[hbm] * 17,
        out_specs=hbm,
        scratch_shapes=[
            vm((BLOCK, wide), BF16),
            vm((rows, depth), BF16),
            vm((depth, 8 * width), BF16),
            vm((7, rows, width), BF16),
            vm((rows, width), F32),
            vm((heads, depth), BF16),
            vm((heads, depth), BF16),
            vm((1, heads), F32),
            vm((1, width), F32),
            vm((kernel, width), BF16),
            vm((32, width), F32),
            vm((1, width), F32),
            vm((1, width), F32),
            vm((NY, 2 * BLOCK, wide), BF16),
            vm((NY, 2 * BLOCK, wide), BF16),
            vm((chunks, 2 * BLOCK, width), BF16),
            vm((rows, width), F32),
            vm((rows, BLOCK), BF16),
            vm((chunks, width, BLOCK), BF16),
            vm((chunks, 8, BLOCK), F32),
            vm((width, 2 * width), F32),
            vm((rows, width), BF16),
            vm((rows, width), F32),
            vm((NX, width, 2 * width), BF16),
            vm((2, width, 2 * width), BF16),
            vm((2, width, 2 * width), BF16),
            vm((width, width), BF16),
            vm((width, width), BF16),
            vm((halo + rows, width), F32),
            vm((rows, width), F32),
            vm((halo, width), BF16),
            vm((halo, width), BF16),
            vm((16, BLOCK), F32),
            vm((7, 16, BLOCK), F32),
            vm((rows, width), BF16),
            vm((7, BLOCK, width), BF16),
            vm((NY, BLOCK, 2 * width), BF16),
            vm((NY, BLOCK, 2 * width), BF16),
            vm((BLOCK, wide), F32),
            vm((rows, width), F32),
            dma((11,)),
            dma((17,)),
            dma((chunks,)),
            dma((chunks,)),
            dma((chunks,)),
            dma((NZ - 1,)),
            dma((13,)),
            dma((5,)),
            dma((5,)),
        ],
        compiler_params=pltpu.CompilerParams(
            collective_id=0, has_side_effects=True, vmem_limit_bytes=60 * 1024 * 1024
        ),
        cost_estimate=pl.CostEstimate(
            flops=10_000_000_000, bytes_accessed=20_000_000, transcendentals=0
        ),
        name="layer",
    )(
        tokens, w_query, w_key, w_value, w_delta_gate, w_glu_value, w_glu_gate, w_conv_gate,
        w_beta.T, w_decay.T, decay_log[None, :], head_gain[None, :], conv_taps,
        ln_gain[None, :], ln_shift[None, :], out_delta, out_conv,
    )


def solution(mesh):
    return jax.shard_map(
        local,
        mesh=mesh,
        in_specs=(
            P("sp", "tp"), P(None, "tp"), P(None, "tp"), P(None, "tp"), P(None, "tp"),
            P(None, "tp"), P(None, "tp"), P(None, "tp"), P(), P(), P(), P(), P(None, "tp"),
            P("tp"), P("tp"), P("tp", None), P("tp", None),
        ),
        out_specs=P(("sp", "tp"), None),
        check_vma=False,
    )
```

```python
import jax
import jax.numpy as jnp
from jax import lax
from jax.experimental import pallas as pl
from jax.experimental.pallas import tpu as pltpu
from jax.sharding import PartitionSpec as P

BLOCK = 128
AHEAD = 4
LAG = 2
TINY_NORM = 1e-06
TINY_VAR = 1e-05
HIGHEST = lax.Precision.HIGHEST
MESH = pl.DeviceIdType.MESH
F32 = jnp.float32
BF16 = jnp.bfloat16
NX = 4
NZ = 8
NY = 4


def nt(a, b):
    return lax.dot_general(a, b, (((1,), (1,)), ((), ())), preferred_element_type=F32)


def mm(a, b):
    return jnp.dot(a.astype(BF16), b.astype(BF16), preferred_element_type=F32)


def compose(later, earlier):
    width = later.shape[0]
    moved = mm(later[:, :width], earlier)
    return jnp.concatenate(
        [moved[:, :width], moved[:, width:] + later[:, width:].astype(F32)], axis=1
    )


def layer_kernel(
    tok_hbm, wq_hbm, wk_hbm, wv_hbm, wdg_hbm, wgv_hbm, wgg_hbm, wcg_hbm, wb_hbm, wdec_hbm,
    rate_hbm, gain_hbm, taps_hbm, lng_hbm, lns_hbm, od_hbm, oc_hbm,
    out_hbm,
    out_ref, full, w_all, proj, gates_ref, wb_s, wdec_s, rate_s, gain_s, taps_s, tapf_s, lng_s, lns_s,
    wd, wc, lhs_s, corr_s, score_s, wt_s, tail_s, state_ref, outa_s, outb_s,
    xin, zs, zr, zs4, zr4, padded, filtered, halo_out, halo_in, sums_out, sums_in,
    cm_s, dsend, in_d, in_c, acc, gate_s,
    l_sem, sent, a_recv, f_recv, b_recv, w2_recv, got, z_send, z_recv,
):
    rows, part = tok_hbm.shape
    chunks = rows // BLOCK
    width = gain_hbm.shape[1]
    halo = halo_in.shape[0]
    kernel = taps_hbm.shape[0]
    sp, place = NX * NZ, lax.axis_index("sp")
    me = lax.axis_index("tp")
    core, y = lax.rem(me, 2), me // 2
    x, z = lax.rem(place, NX), place // NX
    sibling = me + 1 - 2 * core

    def tp_at(o, p=0):
        side = core + p * (1 - 2 * core)
        return lax.rem(y + o + NY, NY) * 2 + side

    def sp_at(dz, dx):
        return lax.rem(z + dz + NZ, NZ) * NX + lax.rem(x + dx + NX, NX)

    barrier = pltpu.get_barrier_semaphore()

    def greet(**device):
        pl.semaphore_signal(barrier, inc=1, device_id=device, device_id_type=MESH)

    for o in (1, 2, 3):
        for p in range(2):
            greet(tp=tp_at(o, p))
    greet(tp=sibling)
    for j in range(1, NZ):
        greet(sp=sp_at(j, 0))
    for k in range(1, NX):
        greet(sp=sp_at(0, k))
    greet(sp=lax.rem(place + sp - 1, sp))

    def columns(owner):
        return pl.ds(pl.multiple_of(owner * part, part), part)

    def at(t):
        return pl.ds(pl.multiple_of(t * BLOCK, BLOCK), BLOCK)

    def load(i, src, dst):
        return pltpu.make_async_copy(src, dst, l_sem.at[i])

    loads = {"tok": load(0, tok_hbm, full.at[:, columns(me)]), "oc": load(1, oc_hbm, wc.at[0, :BLOCK, :])}
    for i, src in enumerate((wq_hbm, wk_hbm, wv_hbm, wdg_hbm, wgv_hbm, wgg_hbm, wcg_hbm)):
        loads[i] = load(2, src, w_all.at[:, i * width : (i + 1) * width])
    loads["wb"] = load(3, wb_hbm, wb_s)
    loads["wdec"] = load(4, wdec_hbm, wdec_s)
    loads["rate"] = load(5, rate_hbm, rate_s)
    loads["gain"] = load(6, gain_hbm, gain_s)
    loads["taps"] = load(7, taps_hbm, taps_s)
    loads["lng"] = load(8, lng_hbm, lng_s)
    loads["lns"] = load(9, lns_hbm, lns_s)
    loads["od"] = load(10, od_hbm, wd.at[0, :BLOCK, :])
    for copy in loads.values():
        copy.start()

    def remote(src, dst, send, recv, **device):
        return pltpu.make_async_remote_copy(
            src_ref=src, dst_ref=dst, send_sem=send, recv_sem=recv,
            device_id=device, device_id_type=MESH,
        )

    def settle(ref, send):
        remote(ref, ref, sent.at[send], got.at[0], tp=sibling).wait_send()

    def landed(ref, recv):
        remote(ref, ref, sent.at[0], recv, tp=sibling).wait_recv()

    def to_right(r):
        block = full.at[at(r), columns(me)]
        return remote(block, block, sent.at[0], a_recv.at[r], tp=tp_at(1))

    def to_left(r):
        block = full.at[at(r), columns(me)]
        return remote(block, block, sent.at[1], a_recv.at[r], tp=tp_at(-1))

    def half(r, i):
        return pl.ds(pl.multiple_of(r * BLOCK + i * (BLOCK // 2), BLOCK // 2), BLOCK // 2)

    def on_right(r):
        block = full.at[half(r, 0), columns(tp_at(-1))]
        return remote(block, block, sent.at[2], f_recv.at[r], tp=tp_at(1))

    def on_left(r):
        block = full.at[half(r, 1), columns(tp_at(1))]
        return remote(block, block, sent.at[3], f_recv.at[r], tp=tp_at(-1))

    def beside(o, r):
        block = full.at[at(r), columns(tp_at(o))]
        return remote(block, block, sent.at[4], b_recv.at[r], tp=sibling)

    zrows = BLOCK // NZ
    xcols = wc.shape[2] // NX

    def wpiece(i):
        return (
            pl.ds(pl.multiple_of(lax.rem(z - i + NZ, NZ) * zrows, zrows), zrows),
            pl.ds(pl.multiple_of(x * xcols, xcols), xcols),
        )

    def w_first(o):
        a, b = wpiece(0)
        return remote(
            wc.at[0, a, b], wc.at[NY - o, a, b], sent.at[5], got.at[1], tp=tp_at(o)
        )

    def w_second(j):
        a, b = wpiece(0)
        block = wc.at[pl.ds(1, NY - 1), a, b]
        return remote(block, block, sent.at[6], w2_recv.at[j - 1], sp=sp_at(j, 0))

    def w_third(i, k):
        a, b = wpiece(i)
        block = wc.at[pl.ds(1, NY - 1), a, b]
        return remote(block, block, sent.at[7], got.at[2], sp=sp_at(0, k))

    def w_beside():
        return remote(
            wc.at[:, pl.ds(0, BLOCK), :], wc.at[:, pl.ds(BLOCK, BLOCK), :],
            sent.at[8], got.at[3], tp=sibling,
        )

    def d_beside(d):
        return remote(
            wd.at[d, pl.ds(0, BLOCK), :], wd.at[d, pl.ds(BLOCK, BLOCK), :],
            sent.at[9], got.at[4], tp=sibling,
        )

    hb = BLOCK // 2

    def d_right(i):
        return remote(
            wd.at[0, pl.ds(i * hb, hb), :], wd.at[3, pl.ds(i * hb, hb), :],
            sent.at[10], got.at[5], tp=tp_at(1),
        )

    def d_left(i):
        return remote(
            wd.at[0, pl.ds((1 - i) * hb, hb), :], wd.at[1, pl.ds((1 - i) * hb, hb), :],
            sent.at[10], got.at[5], tp=tp_at(-1),
        )

    def d_on_right():
        return remote(
            wd.at[3, pl.ds(0, hb), :], wd.at[2, pl.ds(0, hb), :],
            sent.at[11], got.at[6], tp=tp_at(1),
        )

    def d_on_left():
        return remote(
            wd.at[1, pl.ds(hb, hb), :], wd.at[2, pl.ds(hb, hb), :],
            sent.at[11], got.at[6], tp=tp_at(-1),
        )

    loads["tok"].wait()
    loads["oc"].wait()
    pl.semaphore_wait(barrier, 7 + NZ - 1 + NX - 1 + 1)
    for o in (2, 1, 3):
        w_first(o).start()
    for r in range(AHEAD):
        to_right(r).start()
        to_left(r).start()

    def own_beside(r, carry):
        beside(0, r).start()
        return carry

    lax.fori_loop(0, chunks, own_beside, 0)

    loads["wb"].wait()
    loads["wdec"].wait()
    loads["rate"].wait()
    heads = wb_s.shape[0]
    pick = lax.broadcasted_iota(jnp.int32, wb_s.shape, 0) == me
    beta_row = jnp.sum(jnp.where(pick, wb_s[...].astype(F32), 0.0), axis=0, keepdims=True)
    decay_row = jnp.sum(jnp.where(pick, wdec_s[...].astype(F32), 0.0), axis=0, keepdims=True)
    sub_id = lax.broadcasted_iota(jnp.int32, (BLOCK, BLOCK), 0)
    for b in range(2 * NY * part // BLOCK):
        cut = slice(b * BLOCK, (b + 1) * BLOCK)
        tall = jnp.where(sub_id == 0, beta_row[:, cut], jnp.where(sub_id == 1, decay_row[:, cut], 0.0))
        w_all[cut, 7 * width : 8 * width] = tall.T.astype(BF16)
    lane8 = lax.broadcasted_iota(jnp.int32, (1, heads), 1)
    rate = jnp.exp(
        jnp.sum(jnp.where(lane8 == me, rate_s[...], 0.0), axis=1, keepdims=True)
    )
    load(2, w_all.at[:, : 7 * width], w_all.at[:, : 7 * width]).wait()
    loads["taps"].wait()
    tapf_s[:kernel, :] = taps_s[...].astype(F32)

    def arrive(r):
        landed(full.at[at(r), pl.ds(0, 2 * part)], a_recv.at[r])
        on_right(r).start()
        on_left(r).start()
        beside(3, r).start()
        beside(1, r).start()

        if r + AHEAD < chunks:
            to_right(r + AHEAD).start()
            to_left(r + AHEAD).start()

    def arrive_far(r):
        landed(full.at[at(r), pl.ds(0, part)], f_recv.at[r])
        beside(2, r).start()

    def w_pass(r):
        w_second(r).wait_recv()
        for k in (2, 1, 3):
            w_third(r, k).start()

    def chunk_steps(r, count):
        for i in range(count):
            landed(full.at[at(r + i), pl.ds(0, NY * part)], b_recv.at[r + i])
        size = count * BLOCK
        here = pl.ds(pl.multiple_of(r * BLOCK, BLOCK), size)
        squares = jnp.zeros((size, 1), F32)
        for b in range(2 * NY):
            piece = full[here, b * part : (b + 1) * part].astype(F32)
            squares = squares + jnp.sum(piece * piece, axis=1, keepdims=True)
        inv_rms = lax.rsqrt(squares / (part * 2 * NY) + TINY_NORM)
        yield
        for j in range(4):
            summed = jnp.dot(
                full[here, :], w_all[:, j * 256 : (j + 1) * 256], preferred_element_type=F32
            )
            summed = summed * inv_rms
            proj[2 * j, here, :] = summed[:, :width].astype(BF16)
            if j < 3:
                proj[2 * j + 1, here, :] = summed[:, width:].astype(BF16)
            else:
                raw = summed[:, width:]
                lane = lax.broadcasted_iota(jnp.int32, raw.shape, 1)
                softplus = jnp.maximum(raw, 0.0) + jnp.log1p(jnp.exp(-jnp.abs(raw)))
                gates_ref[here, :] = jnp.where(
                    lane == 0, jax.nn.sigmoid(raw), jnp.where(lane == 1, -rate * softplus, 0.0)
                )
            yield

    def chunk(r, count):
        list(chunk_steps(r, count))

    def take(steps, count):
        for _ in range(count):
            next(steps)

    row_id = lax.broadcasted_iota(jnp.int32, (BLOCK, BLOCK), 0)
    col_id = lax.broadcasted_iota(jnp.int32, (BLOCK, BLOCK), 1)
    causal = row_id >= col_id
    strict = row_id > col_id
    differ = row_id ^ col_id
    eye = jnp.where(row_id == col_id, 1.0, 0.0)
    tril = jnp.where(causal, 1.0, 0.0)
    ident = jnp.concatenate([eye, jnp.zeros((width, width), F32)], axis=1)

    def prepare(c):
        here = slice(c * BLOCK, (c + 1) * BLOCK)
        gates = gates_ref[here, :]
        sums = jnp.dot(tril, gates, precision=HIGHEST, preferred_element_type=F32)
        q, k = proj[0, here, :], proj[1, here, :]
        v = proj[2, here, :].astype(F32)
        kf, qf = k.astype(F32), q.astype(F32)
        ik = lax.rsqrt(jnp.sum(kf * kf, axis=-1, keepdims=True) + TINY_NORM)
        iq = lax.rsqrt(jnp.sum(qf * qf, axis=-1, keepdims=True) + TINY_NORM)
        iq = iq * width ** (-0.5)
        beta = gates[:, 0:1]
        log_sum = sums[:, 1:2]
        log_full = jnp.broadcast_to(log_sum, (BLOCK, BLOCK))
        spread = log_full - log_full.T
        damp = jnp.where(causal, jnp.exp(jnp.where(causal, spread, 0.0)), 0.0)
        damp = damp * jnp.broadcast_to(ik, (BLOCK, BLOCK)).T
        lower = jnp.where(strict, nt(k, k) * damp * (beta * ik), 0.0)
        score_s[here, :] = (nt(q, k) * damp * iq).astype(BF16)
        grow = jnp.exp(log_sum)
        right = jnp.concatenate([v * beta, kf * (beta * ik * grow)], axis=1)
        tail = log_full[BLOCK - 1 : BLOCK, :]
        weighted = kf * (ik * jnp.exp(tail[:, :1] - log_sum))
        wt_s[c] = weighted.T.astype(BF16)
        tail_s[c] = jnp.broadcast_to(jnp.exp(tail), (8, BLOCK))
        lhs_s[c, BLOCK:, :] = (qf * (iq * grow)).astype(BF16)
        return [c, lower, right, eye - jnp.where(differ == 1, lower, 0.0)]

    def advance(c, carry):
        both = mm(lhs_s[c], state_ref[...])
        first = both[:BLOCK]
        fresh = jnp.concatenate(
            [-first[:, :width], corr_s[at(c), :] - first[:, width:]], axis=1
        ).astype(BF16)
        decay = tail_s[c][:1, :]
        decay = jnp.concatenate([decay, decay], axis=1)
        state_ref[...] = state_ref[...] * decay + mm(wt_s[c], fresh)
        out = both[BLOCK:] + mm(score_s[at(c), :], fresh)
        outa_s[at(c), :] = out[:, :width].astype(BF16)
        outb_s[at(c), :] = out[:, width:]
        return carry

    def delta_group(first, count, until):
        chains = [prepare(first + i) for i in range(count)]
        yield
        size = 2
        while size < BLOCK:
            level = (differ >= size) & (differ < 4 * size)
            steps = [mm(ch[3], jnp.where(level, ch[1], 0.0)) for ch in chains]
            yield
            once = [ch[3] - mm(step, ch[3]) for ch, step in zip(chains, steps)]
            twice = [mm(step, step) for step in steps]
            yield
            for ch, one, two in zip(chains, once, twice):
                ch[3] = one + mm(two, one)
            size *= 4
            yield
        for c, lower, right, inverse in chains:
            solved = mm(inverse, right)
            corr_s[c * BLOCK : (c + 1) * BLOCK, :] = solved[:, :width]
            lhs_s[c, :BLOCK, :] = solved[:, width:].astype(BF16)
        lax.fori_loop(first, until, advance, 0)

    state_ref[...] = ident
    landed(wc.at[0, pl.ds(0, 3 * zrows), pl.ds(0, xcols)], got.at[1])
    for j in range(1, NZ):
        w_second(j).start()
    for k in (2, 1, 3):
        w_third(0, k).start()
    early = delta_group(0, 4, 2)
    for t in range(chunks + LAG):
        if t < chunks:
            arrive(t)
        if t == chunks - 1:
            loads["od"].wait()
            for i in range(2):
                d_right(i).start()
                d_left(i).start()
        if 1 <= t < NZ:
            w_pass(t)
        k = t - LAG
        if k < 0:
            continue
        arrive_far(k)
        if k == 2 or k == 4:
            chunk(k - 2, 2)
        if k == 5:
            take(early, 4)
        if k == 6:
            woven = chunk_steps(4, 2)
            for _ in range(5):
                next(woven)
                next(early)
            list(woven)
            next(early)
    list(early)
    chunk(6, 2)

    def unit(t):
        value = proj[4, at(t), :].astype(F32)
        units = (value * jax.nn.sigmoid(proj[5, at(t), :].astype(F32))).astype(BF16)
        padded[pl.ds(pl.multiple_of(t * BLOCK + halo, halo), BLOCK), :] = units.astype(F32)
        return units

    units = unit(chunks - 1)
    halo_out[...] = units[BLOCK - halo :, :]
    halo_copy = remote(
        halo_out, halo_in, sent.at[13], got.at[8], sp=lax.rem(place + 1, sp)
    )

    @pl.when(place + 1 < sp)
    def _():
        halo_copy.start()

    late = delta_group(4, 4, 8)
    take(late, 2)
    advance(2, 0)
    take(late, 3)
    advance(3, 0)
    list(late)

    xin[0] = state_ref[...].astype(BF16)

    def x_copy(k):
        return remote(xin.at[0], xin.at[k], sent.at[12], got.at[7], sp=sp_at(0, k))

    for k in (2, 1, 3):
        x_copy(k).start()

    def unit_loop(t, carry):
        unit(t)
        return carry

    landed(wc.at[pl.ds(1, NY - 1), pl.ds(0, 96), :], got.at[2])
    w_beside().start()
    lax.fori_loop(0, chunks - 1, unit_loop, 0)

    def conv(t, carry):
        total = jnp.zeros((BLOCK, width), F32)
        for j in range(kernel):
            start = t * BLOCK + (halo - kernel + 1 + j)
            total = total + padded[pl.ds(start, BLOCK), :] * tapf_s[j : j + 1, :]
        filtered[at(t), :] = total
        first = jnp.sum(total, axis=1, keepdims=True)
        second = jnp.sum(total * total, axis=1, keepdims=True)
        turned = jnp.where(col_id == 0, first, jnp.where(col_id == 1, second, 0.0)).T
        sums_out[pl.ds(t, 1), :] = turned[0:1, :]
        sums_out[pl.ds(t + 8, 1), :] = turned[1:2, :]
        return carry

    lax.fori_loop(1, chunks, conv, 0)

    @pl.when(place >= 1)
    def _():
        halo_copy.wait_recv()

    @pl.when(place < 1)
    def _():
        halo_in[...] = jnp.zeros(halo_in.shape, BF16)

    padded[:halo, :] = halo_in[...].astype(F32)
    conv(0, 0)

    def ln_copy(o, p):
        i = 2 * o + p - 1
        return remote(sums_out, sums_in.at[i], sent.at[14], got.at[9], tp=tp_at(o, p))

    others = [(2, 0), (2, 1), (1, 0), (1, 1), (3, 0), (3, 1), (0, 1)]
    for o, p in others:
        ln_copy(o, p).start()
    landed(wd.at[pl.ds(0, 2), pl.ds(0, BLOCK), :], got.at[5])
    d_on_right().start()
    d_on_left().start()
    for d in (0, 1, 3):
        d_beside(d).start()

    landed(xin.at[pl.ds(1, NX - 1)], got.at[7])

    def piece(i):
        return xin[lax.rem(x - i + NX, NX)]

    p0, p1, p2, p3 = (piece(i) for i in range(NX))
    w2 = compose(p1, p0)
    pair = compose(p3, p2)
    group = compose(pair, w2)
    w3 = compose(p2, w2)
    inner = jnp.where(
        x == 0, ident, jnp.where(x == 1, p0.astype(F32), jnp.where(x == 2, w2, w3))
    ).astype(BF16)
    zs[0] = group.astype(BF16)

    def z_copy(i, b):
        cut = pl.ds(b * width, width)
        return remote(
            zs.at[i, :, cut], zr.at[i, :, cut],
            z_send.at[2 * i + b], z_recv.at[2 * i + b], sp=sp_at(i + 1, 0),
        )

    last_copy = remote(zs4, zr4, z_send.at[4], z_recv.at[4], sp=sp_at(4, 0))

    def z_start(i, b):
        @pl.when(z + i + 1 < NZ)
        def _():
            z_copy(i, b).start()

    def z_wait(i, b):
        @pl.when(z >= i + 1)
        def _():
            z_copy(i, b).wait_recv()

    z_start(0, 1)
    z_start(0, 0)

    for i in range(2):

        @pl.when(z < i + 1)
        def _(i=i):
            zr[i] = ident.astype(BF16)

    @pl.when(z < 4)
    def _():
        zr4[...] = jnp.zeros(zr4.shape, BF16)

    settle(full.at[:, columns(me)], 0)
    settle(full.at[:, columns(me)], 1)
    settle(full.at[pl.ds(0, rows // 2), columns(me)], 2)
    settle(full.at[pl.ds(0, rows // 2), columns(me)], 3)
    settle(full.at[:, pl.ds(0, NY * part)], 4)
    settle(wc.at[0, pl.ds(0, 3 * zrows), pl.ds(0, xcols)], 5)
    settle(wc.at[pl.ds(1, NY - 1), pl.ds(0, 7 * zrows), pl.ds(0, xcols)], 6)
    settle(wc.at[pl.ds(1, NY - 1), pl.ds(0, 96), :], 7)
    settle(xin.at[pl.ds(1, NX - 1)], 12)

    def left(i):
        return zs[i][:, :width]

    z_wait(0, 1)
    zs[1, :, width:] = (
        mm(left(0), zr[0, :, width:]) + zs[0, :, width:].astype(F32)
    ).astype(BF16)
    z_start(1, 1)
    z_wait(0, 0)
    e1 = zr[0]
    zs[1, :, :width] = mm(left(0), e1[:, :width]).astype(BF16)
    z_start(1, 0)

    landed(sums_in, got.at[9])
    loads["lng"].wait()
    loads["lns"].wait()
    loads["gain"].wait()
    sums = sums_out[...]
    for i in range(7):
        sums = sums + sums_in[i]
    sums = jnp.concatenate([sums, jnp.zeros((BLOCK - 16, BLOCK), F32)], axis=0).T
    channels = width * 2 * NY
    center_all = sums[:, 0:8] / channels
    variance = jnp.maximum(sums[:, 8:16] / channels - center_all * center_all, 0.0)
    scale_all = lax.rsqrt(variance + TINY_VAR)
    for t in range(chunks):
        here = slice(t * BLOCK, (t + 1) * BLOCK)
        normed = (filtered[here, :] - center_all[:, t : t + 1]) * scale_all[:, t : t + 1]
        normed = normed * lng_s[...] + lns_s[...]
        gate = proj[6, here, :].astype(F32)
        cm_s[here, :] = (jax.nn.silu(normed) * jax.nn.silu(gate)).astype(BF16)

    def c_copy(o, p):
        i = 2 * o + p - 1
        return remote(
            cm_s.at[at(tp_at(o, p)), :],
            in_c.at[(NY - o) % NY, :, pl.ds(p * width, width)],
            sent.at[15], got.at[10], tp=tp_at(o, p),
        )

    for o, p in others:
        c_copy(o, p).start()
    in_c[0, :, :width] = cm_s[at(me), :]
    z_wait(1, 1)
    zs4[...] = (mm(left(1), zr[1, :, width:]) + zs[1, :, width:].astype(F32)).astype(BF16)

    @pl.when(z + 4 < NZ)
    def _():
        last_copy.start()

    landed(wd.at[0, pl.ds(0, BLOCK), :], got.at[6])
    d_beside(2).start()
    z_wait(1, 0)
    e3 = compose(e1, zr[1])
    reach = compose(inner, e3)

    for t in range(chunks):
        here = slice(t * BLOCK, (t + 1) * BLOCK)
        gate_s[here, :] = gain_s[...] * jax.nn.silu(proj[3, here, :].astype(F32))

    w_beside().wait_recv()
    landed(dsend, got.at[10])
    step = 512
    cuts = out_ref.shape[1] // step

    def out_copy(n):
        cut = pl.ds(n * step, step)
        return pltpu.make_async_copy(out_ref.at[:, cut], out_hbm.at[:, cut], l_sem.at[0])

    for n in range(cuts):
        cut = slice(n * step, (n + 1) * step)
        total = jnp.zeros((BLOCK, step), F32)
        for d in range(NY):
            total = total + jnp.dot(in_c[d], wc[d, :, cut], preferred_element_type=F32)
        acc[:, cut] = total

    @pl.when(z >= 4)
    def _():
        last_copy.wait_recv()

    carried = (mm(reach[:, :width], zr4[...]) + reach[:, width:]).astype(BF16)

    def d_copy(o, p):
        i = 2 * o + p - 1
        return remote(
            dsend.at[i], in_d.at[(NY - o) % NY, :, pl.ds(p * width, width)],
            sent.at[16], got.at[0 if o == 0 else 11 if o == 2 else 12], tp=tp_at(o, p),
        )

    for batch in (others[:2], others[2:6], [(0, 1), (0, 0)]):
        places = [at(tp_at(o, p)) for o, p in batch]
        results = [outb_s[pos, :] + mm(outa_s[pos, :], carried) for pos in places]
        scales = [
            lax.rsqrt(jnp.mean(res * res, axis=-1, keepdims=True) + TINY_NORM) for res in results
        ]
        mixed = [
            (res * sc * gate_s[pos, :]).astype(BF16)
            for res, sc, pos in zip(results, scales, places)
        ]
        for (o, p), value in zip(batch, mixed):
            if o == 0 and p == 0:
                in_d[0, :, :width] = value
            else:
                dsend[2 * o + p - 1] = value
        for o, p in batch:
            if o or p:
                d_copy(o, p).start()

    landed(wd.at[:, pl.ds(0, BLOCK), :], got.at[4])
    for group_at, count, sem in (((0,), 1, 0), ((3, 1), 4, 12), ((2,), 2, 11)):
        landed(dsend.at[pl.ds(0, count)], got.at[sem])
        for n in range(cuts):
            cut = slice(n * step, (n + 1) * step)
            total = acc[:, cut]
            for d in group_at:
                total = total + jnp.dot(in_d[d], wd[d, :, cut], preferred_element_type=F32)
            if group_at == (2,):
                out_ref[:, cut] = total.astype(BF16)
                out_copy(n).start()
            else:
                acc[:, cut] = total

    settle(wc.at[:, pl.ds(0, BLOCK), :], 8)
    settle(wd.at[:, pl.ds(0, BLOCK), :], 9)
    settle(wd.at[pl.ds(0, 2), pl.ds(0, BLOCK), :], 10)
    settle(wd.at[0, pl.ds(0, BLOCK), :], 11)

    @pl.when(place + 1 < sp)
    def _():
        halo_copy.wait_send()

    for i in range(2):

        @pl.when(z + i + 1 < NZ)
        def _(i=i):
            z_copy(i, 0).wait_send()
            z_copy(i, 1).wait_send()

    @pl.when(z + 4 < NZ)
    def _():
        last_copy.wait_send()

    settle(sums_in, 14)
    settle(dsend, 15)
    settle(dsend, 16)
    pltpu.make_async_copy(out_ref, out_hbm, l_sem.at[0]).wait()


def local(
    tokens, w_query, w_key, w_value, w_delta_gate, w_glu_value, w_glu_gate, w_conv_gate,
    w_beta, w_decay, decay_log, head_gain, conv_taps, ln_gain, ln_shift, out_delta, out_conv,
):
    rows, part = tokens.shape
    depth, width = w_query.shape
    wide = out_delta.shape[1]
    heads = w_beta.shape[1]
    chunks = rows // BLOCK
    kernel = conv_taps.shape[0]
    halo = (kernel - 1 + 31) // 32 * 32
    hbm = pl.BlockSpec(memory_space=pltpu.HBM)
    dma = pltpu.SemaphoreType.DMA
    vm = pltpu.VMEM
    return pl.pallas_call(
        layer_kernel,
        out_shape=jax.ShapeDtypeStruct((BLOCK, wide), BF16),
        in_specs=[hbm] * 17,
        out_specs=hbm,
        scratch_shapes=[
            vm((BLOCK, wide), BF16),
            vm((rows, depth), BF16),
            vm((depth, 8 * width), BF16),
            vm((7, rows, width), BF16),
            vm((rows, width), F32),
            vm((heads, depth), BF16),
            vm((heads, depth), BF16),
            vm((1, heads), F32),
            vm((1, width), F32),
            vm((kernel, width), BF16),
            vm((32, width), F32),
            vm((1, width), F32),
            vm((1, width), F32),
            vm((NY, 2 * BLOCK, wide), BF16),
            vm((NY, 2 * BLOCK, wide), BF16),
            vm((chunks, 2 * BLOCK, width), BF16),
            vm((rows, width), F32),
            vm((rows, BLOCK), BF16),
            vm((chunks, width, BLOCK), BF16),
            vm((chunks, 8, BLOCK), F32),
            vm((width, 2 * width), F32),
            vm((rows, width), BF16),
            vm((rows, width), F32),
            vm((NX, width, 2 * width), BF16),
            vm((2, width, 2 * width), BF16),
            vm((2, width, 2 * width), BF16),
            vm((width, width), BF16),
            vm((width, width), BF16),
            vm((halo + rows, width), F32),
            vm((rows, width), F32),
            vm((halo, width), BF16),
            vm((halo, width), BF16),
            vm((16, BLOCK), F32),
            vm((7, 16, BLOCK), F32),
            vm((rows, width), BF16),
            vm((7, BLOCK, width), BF16),
            vm((NY, BLOCK, 2 * width), BF16),
            vm((NY, BLOCK, 2 * width), BF16),
            vm((BLOCK, wide), F32),
            vm((rows, width), F32),
            dma((11,)),
            dma((17,)),
            dma((chunks,)),
            dma((chunks,)),
            dma((chunks,)),
            dma((NZ - 1,)),
            dma((13,)),
            dma((5,)),
            dma((5,)),
        ],
        compiler_params=pltpu.CompilerParams(
            collective_id=0, has_side_effects=True, vmem_limit_bytes=60 * 1024 * 1024
        ),
        cost_estimate=pl.CostEstimate(
            flops=10_000_000_000, bytes_accessed=20_000_000, transcendentals=0
        ),
        name="layer",
    )(
        tokens, w_query, w_key, w_value, w_delta_gate, w_glu_value, w_glu_gate, w_conv_gate,
        w_beta.T, w_decay.T, decay_log[None, :], head_gain[None, :], conv_taps,
        ln_gain[None, :], ln_shift[None, :], out_delta, out_conv,
    )


def solution(mesh):
    return jax.shard_map(
        local,
        mesh=mesh,
        in_specs=(
            P("sp", "tp"), P(None, "tp"), P(None, "tp"), P(None, "tp"), P(None, "tp"),
            P(None, "tp"), P(None, "tp"), P(None, "tp"), P(), P(), P(), P(), P(None, "tp"),
            P("tp"), P("tp"), P("tp", None), P("tp", None),
        ),
        out_specs=P(("sp", "tp"), None),
        check_vma=False,
    )
```

```python
import jax
import jax.numpy as jnp
from jax import lax
from jax.experimental import pallas as pl
from jax.experimental.pallas import tpu as pltpu
from jax.sharding import PartitionSpec as P

BLOCK = 128
AHEAD = 4
LAG = 3
TINY_NORM = 1e-06
TINY_VAR = 1e-05
HIGHEST = lax.Precision.HIGHEST
MESH = pl.DeviceIdType.MESH
F32 = jnp.float32
BF16 = jnp.bfloat16
NX = 4
NZ = 8
NY = 4


def nt(a, b):
    return lax.dot_general(a, b, (((1,), (1,)), ((), ())), preferred_element_type=F32)


def mm(a, b):
    return jnp.dot(a.astype(BF16), b.astype(BF16), preferred_element_type=F32)


def compose(later, earlier):
    width = later.shape[0]
    moved = mm(later[:, :width], earlier)
    return jnp.concatenate(
        [moved[:, :width], moved[:, width:] + later[:, width:].astype(F32)], axis=1
    )


def layer_kernel(
    tok_hbm, wq_hbm, wk_hbm, wv_hbm, wdg_hbm, wgv_hbm, wgg_hbm, wcg_hbm, wb_hbm, wdec_hbm,
    rate_hbm, gain_hbm, taps_hbm, lng_hbm, lns_hbm, od_hbm, oc_hbm,
    out_hbm,
    out_ref, full, w_all, proj, gates_ref, wb_s, wdec_s, rate_s, gain_s, taps_s, tapf_s, lng_s, lns_s,
    wd, wc, lhs_s, corr_s, score_s, wt_s, tail_s, state_ref, outa_s, outb_s,
    xin, zs, zr, zs4, zr4, padded, filtered, halo_out, halo_in, sums_out, sums_in,
    cm_s, dsend, in_d, in_c, acc, gate_s,
    l_sem, sent, a_recv, f_recv, b_recv, w2_recv, got, z_send, z_recv,
):
    rows, part = tok_hbm.shape
    chunks = rows // BLOCK
    width = gain_hbm.shape[1]
    halo = halo_in.shape[0]
    kernel = taps_hbm.shape[0]
    sp, place = NX * NZ, lax.axis_index("sp")
    me = lax.axis_index("tp")
    core, y = lax.rem(me, 2), me // 2
    x, z = lax.rem(place, NX), place // NX
    sibling = me + 1 - 2 * core

    def tp_at(o, p=0):
        side = core + p * (1 - 2 * core)
        return lax.rem(y + o + NY, NY) * 2 + side

    def sp_at(dz, dx):
        return lax.rem(z + dz + NZ, NZ) * NX + lax.rem(x + dx + NX, NX)

    barrier = pltpu.get_barrier_semaphore()

    def greet(**device):
        pl.semaphore_signal(barrier, inc=1, device_id=device, device_id_type=MESH)

    for o in (1, 2, 3):
        for p in range(2):
            greet(tp=tp_at(o, p))
    greet(tp=sibling)
    for j in range(1, NZ):
        greet(sp=sp_at(j, 0))
    for k in range(1, NX):
        greet(sp=sp_at(0, k))
    greet(sp=lax.rem(place + sp - 1, sp))

    def columns(owner):
        return pl.ds(pl.multiple_of(owner * part, part), part)

    def at(t):
        return pl.ds(pl.multiple_of(t * BLOCK, BLOCK), BLOCK)

    def load(i, src, dst):
        return pltpu.make_async_copy(src, dst, l_sem.at[i])

    loads = {"tok": load(0, tok_hbm, full.at[:, columns(me)]), "oc": load(1, oc_hbm, wc.at[0, :BLOCK, :])}
    for i, src in enumerate((wq_hbm, wk_hbm, wv_hbm, wdg_hbm, wgv_hbm, wgg_hbm, wcg_hbm)):
        loads[i] = load(2, src, w_all.at[:, i * width : (i + 1) * width])
    loads["wb"] = load(3, wb_hbm, wb_s)
    loads["wdec"] = load(4, wdec_hbm, wdec_s)
    loads["rate"] = load(5, rate_hbm, rate_s)
    loads["gain"] = load(6, gain_hbm, gain_s)
    loads["taps"] = load(7, taps_hbm, taps_s)
    loads["lng"] = load(8, lng_hbm, lng_s)
    loads["lns"] = load(9, lns_hbm, lns_s)
    loads["od"] = load(10, od_hbm, wd.at[0, :BLOCK, :])
    for copy in loads.values():
        copy.start()

    def remote(src, dst, send, recv, **device):
        return pltpu.make_async_remote_copy(
            src_ref=src, dst_ref=dst, send_sem=send, recv_sem=recv,
            device_id=device, device_id_type=MESH,
        )

    def settle(ref, send):
        remote(ref, ref, sent.at[send], got.at[0], tp=sibling).wait_send()

    def landed(ref, recv):
        remote(ref, ref, sent.at[0], recv, tp=sibling).wait_recv()

    def to_right(r):
        block = full.at[at(r), columns(me)]
        return remote(block, block, sent.at[0], a_recv.at[r], tp=tp_at(1))

    def to_left(r):
        block = full.at[at(r), columns(me)]
        return remote(block, block, sent.at[1], a_recv.at[r], tp=tp_at(-1))

    def half(r, i):
        return pl.ds(pl.multiple_of(r * BLOCK + i * (BLOCK // 2), BLOCK // 2), BLOCK // 2)

    def on_right(r):
        block = full.at[half(r, 0), columns(tp_at(-1))]
        return remote(block, block, sent.at[2], f_recv.at[r], tp=tp_at(1))

    def on_left(r):
        block = full.at[half(r, 1), columns(tp_at(1))]
        return remote(block, block, sent.at[3], f_recv.at[r], tp=tp_at(-1))

    def beside(o, r):
        block = full.at[at(r), columns(tp_at(o))]
        return remote(block, block, sent.at[4], b_recv.at[r], tp=sibling)

    zrows = BLOCK // NZ
    xcols = wc.shape[2] // NX

    def wpiece(i):
        return (
            pl.ds(pl.multiple_of(lax.rem(z - i + NZ, NZ) * zrows, zrows), zrows),
            pl.ds(pl.multiple_of(x * xcols, xcols), xcols),
        )

    def w_first(o):
        a, b = wpiece(0)
        return remote(
            wc.at[0, a, b], wc.at[NY - o, a, b], sent.at[5], got.at[1], tp=tp_at(o)
        )

    def w_second(j):
        a, b = wpiece(0)
        block = wc.at[pl.ds(1, NY - 1), a, b]
        return remote(block, block, sent.at[6], w2_recv.at[j - 1], sp=sp_at(j, 0))

    def w_third(i, k):
        a, b = wpiece(i)
        block = wc.at[pl.ds(1, NY - 1), a, b]
        return remote(block, block, sent.at[7], got.at[2], sp=sp_at(0, k))

    def w_beside():
        return remote(
            wc.at[:, pl.ds(0, BLOCK), :], wc.at[:, pl.ds(BLOCK, BLOCK), :],
            sent.at[8], got.at[3], tp=sibling,
        )

    def d_beside(d):
        return remote(
            wd.at[d, pl.ds(0, BLOCK), :], wd.at[d, pl.ds(BLOCK, BLOCK), :],
            sent.at[9], got.at[4], tp=sibling,
        )

    hb = BLOCK // 2

    def d_right(i):
        return remote(
            wd.at[0, pl.ds(i * hb, hb), :], wd.at[3, pl.ds(i * hb, hb), :],
            sent.at[10], got.at[5], tp=tp_at(1),
        )

    def d_left(i):
        return remote(
            wd.at[0, pl.ds((1 - i) * hb, hb), :], wd.at[1, pl.ds((1 - i) * hb, hb), :],
            sent.at[10], got.at[5], tp=tp_at(-1),
        )

    def d_on_right():
        return remote(
            wd.at[3, pl.ds(0, hb), :], wd.at[2, pl.ds(0, hb), :],
            sent.at[11], got.at[6], tp=tp_at(1),
        )

    def d_on_left():
        return remote(
            wd.at[1, pl.ds(hb, hb), :], wd.at[2, pl.ds(hb, hb), :],
            sent.at[11], got.at[6], tp=tp_at(-1),
        )

    loads["tok"].wait()
    loads["oc"].wait()
    pl.semaphore_wait(barrier, 7 + NZ - 1 + NX - 1 + 1)
    for o in (2, 1, 3):
        w_first(o).start()
    for r in range(AHEAD):
        to_right(r).start()
        to_left(r).start()

    def own_beside(r, carry):
        beside(0, r).start()
        return carry

    lax.fori_loop(0, chunks, own_beside, 0)

    loads["wb"].wait()
    loads["wdec"].wait()
    loads["rate"].wait()
    heads = wb_s.shape[0]
    pick = lax.broadcasted_iota(jnp.int32, wb_s.shape, 0) == me
    beta_row = jnp.sum(jnp.where(pick, wb_s[...].astype(F32), 0.0), axis=0, keepdims=True)
    decay_row = jnp.sum(jnp.where(pick, wdec_s[...].astype(F32), 0.0), axis=0, keepdims=True)
    sub_id = lax.broadcasted_iota(jnp.int32, (BLOCK, BLOCK), 0)
    for b in range(2 * NY * part // BLOCK):
        cut = slice(b * BLOCK, (b + 1) * BLOCK)
        tall = jnp.where(sub_id == 0, beta_row[:, cut], jnp.where(sub_id == 1, decay_row[:, cut], 0.0))
        w_all[cut, 7 * width : 8 * width] = tall.T.astype(BF16)
    lane8 = lax.broadcasted_iota(jnp.int32, (1, heads), 1)
    rate = jnp.exp(
        jnp.sum(jnp.where(lane8 == me, rate_s[...], 0.0), axis=1, keepdims=True)
    )
    load(2, w_all.at[:, : 7 * width], w_all.at[:, : 7 * width]).wait()
    loads["taps"].wait()
    tapf_s[:kernel, :] = taps_s[...].astype(F32)

    def arrive(r):
        landed(full.at[at(r), pl.ds(0, 2 * part)], a_recv.at[r])
        on_right(r).start()
        on_left(r).start()
        beside(3, r).start()
        beside(1, r).start()

        if r + AHEAD < chunks:
            to_right(r + AHEAD).start()
            to_left(r + AHEAD).start()

    def arrive_far(r):
        landed(full.at[at(r), pl.ds(0, part)], f_recv.at[r])
        beside(2, r).start()

    def w_pass(r):
        w_second(r).wait_recv()
        for k in (2, 1, 3):
            w_third(r, k).start()

    def chunk_steps(r, count):
        for i in range(count):
            landed(full.at[at(r + i), pl.ds(0, NY * part)], b_recv.at[r + i])
        size = count * BLOCK
        here = pl.ds(pl.multiple_of(r * BLOCK, BLOCK), size)
        squares = jnp.zeros((size, 1), F32)
        for b in range(2 * NY):
            piece = full[here, b * part : (b + 1) * part].astype(F32)
            squares = squares + jnp.sum(piece * piece, axis=1, keepdims=True)
        inv_rms = lax.rsqrt(squares / (part * 2 * NY) + TINY_NORM)
        yield
        for j in range(4):
            summed = jnp.dot(
                full[here, :], w_all[:, j * 256 : (j + 1) * 256], preferred_element_type=F32
            )
            summed = summed * inv_rms
            proj[2 * j, here, :] = summed[:, :width].astype(BF16)
            if j < 3:
                proj[2 * j + 1, here, :] = summed[:, width:].astype(BF16)
            else:
                raw = summed[:, width:]
                lane = lax.broadcasted_iota(jnp.int32, raw.shape, 1)
                softplus = jnp.maximum(raw, 0.0) + jnp.log1p(jnp.exp(-jnp.abs(raw)))
                gates_ref[here, :] = jnp.where(
                    lane == 0, jax.nn.sigmoid(raw), jnp.where(lane == 1, -rate * softplus, 0.0)
                )
            yield

    def chunk(r, count):
        list(chunk_steps(r, count))

    def take(steps, count):
        for _ in range(count):
            next(steps)

    row_id = lax.broadcasted_iota(jnp.int32, (BLOCK, BLOCK), 0)
    col_id = lax.broadcasted_iota(jnp.int32, (BLOCK, BLOCK), 1)
    causal = row_id >= col_id
    strict = row_id > col_id
    differ = row_id ^ col_id
    eye = jnp.where(row_id == col_id, 1.0, 0.0)
    tril = jnp.where(causal, 1.0, 0.0)
    ident = jnp.concatenate([eye, jnp.zeros((width, width), F32)], axis=1)

    def prepare(c):
        here = slice(c * BLOCK, (c + 1) * BLOCK)
        gates = gates_ref[here, :]
        sums = jnp.dot(tril, gates, precision=HIGHEST, preferred_element_type=F32)
        q, k = proj[0, here, :], proj[1, here, :]
        v = proj[2, here, :].astype(F32)
        kf, qf = k.astype(F32), q.astype(F32)
        ik = lax.rsqrt(jnp.sum(kf * kf, axis=-1, keepdims=True) + TINY_NORM)
        iq = lax.rsqrt(jnp.sum(qf * qf, axis=-1, keepdims=True) + TINY_NORM)
        iq = iq * width ** (-0.5)
        beta = gates[:, 0:1]
        log_sum = sums[:, 1:2]
        log_full = jnp.broadcast_to(log_sum, (BLOCK, BLOCK))
        spread = log_full - log_full.T
        damp = jnp.where(causal, jnp.exp(jnp.where(causal, spread, 0.0)), 0.0)
        damp = damp * jnp.broadcast_to(ik, (BLOCK, BLOCK)).T
        lower = jnp.where(strict, nt(k, k) * damp * (beta * ik), 0.0)
        score_s[here, :] = (nt(q, k) * damp * iq).astype(BF16)
        grow = jnp.exp(log_sum)
        right = jnp.concatenate([v * beta, kf * (beta * ik * grow)], axis=1)
        tail = log_full[BLOCK - 1 : BLOCK, :]
        weighted = kf * (ik * jnp.exp(tail[:, :1] - log_sum))
        wt_s[c] = weighted.T.astype(BF16)
        tail_s[c] = jnp.broadcast_to(jnp.exp(tail), (8, BLOCK))
        lhs_s[c, BLOCK:, :] = (qf * (iq * grow)).astype(BF16)
        return [c, lower, right, eye - jnp.where(differ == 1, lower, 0.0)]

    def advance(c, carry):
        both = mm(lhs_s[c], state_ref[...])
        first = both[:BLOCK]
        fresh = jnp.concatenate(
            [-first[:, :width], corr_s[at(c), :] - first[:, width:]], axis=1
        ).astype(BF16)
        decay = tail_s[c][:1, :]
        decay = jnp.concatenate([decay, decay], axis=1)
        state_ref[...] = state_ref[...] * decay + mm(wt_s[c], fresh)
        out = both[BLOCK:] + mm(score_s[at(c), :], fresh)
        outa_s[at(c), :] = out[:, :width].astype(BF16)
        outb_s[at(c), :] = out[:, width:]
        return carry

    def delta_group(first, count, until):
        chains = [prepare(first + i) for i in range(count)]
        yield
        size = 2
        while size < BLOCK:
            level = (differ >= size) & (differ < 4 * size)
            steps = [mm(ch[3], jnp.where(level, ch[1], 0.0)) for ch in chains]
            yield
            once = [ch[3] - mm(step, ch[3]) for ch, step in zip(chains, steps)]
            twice = [mm(step, step) for step in steps]
            yield
            for ch, one, two in zip(chains, once, twice):
                ch[3] = one + mm(two, one)
            size *= 4
            yield
        for c, lower, right, inverse in chains:
            solved = mm(inverse, right)
            corr_s[c * BLOCK : (c + 1) * BLOCK, :] = solved[:, :width]
            lhs_s[c, :BLOCK, :] = solved[:, width:].astype(BF16)
        lax.fori_loop(first, until, advance, 0)

    state_ref[...] = ident
    landed(wc.at[0, pl.ds(0, 3 * zrows), pl.ds(0, xcols)], got.at[1])
    for j in range(1, NZ):
        w_second(j).start()
    for k in (2, 1, 3):
        w_third(0, k).start()
    early = delta_group(0, 4, 2)
    for t in range(chunks + LAG):
        if t < chunks:
            arrive(t)
        if t == chunks - 1:
            loads["od"].wait()
            for i in range(2):
                d_right(i).start()
                d_left(i).start()
        if 1 <= t < NZ:
            w_pass(t)
        k = t - LAG
        if k < 0:
            continue
        arrive_far(k)
        if k == 2 or k == 4:
            chunk(k - 2, 2)
        if k == 5:
            take(early, 4)
        if k == 6:
            woven = chunk_steps(4, 2)
            for _ in range(5):
                next(woven)
                next(early)
            list(woven)
            next(early)
    list(early)
    chunk(6, 2)

    def unit(t):
        value = proj[4, at(t), :].astype(F32)
        units = (value * jax.nn.sigmoid(proj[5, at(t), :].astype(F32))).astype(BF16)
        padded[pl.ds(pl.multiple_of(t * BLOCK + halo, halo), BLOCK), :] = units.astype(F32)
        return units

    units = unit(chunks - 1)
    halo_out[...] = units[BLOCK - halo :, :]
    halo_copy = remote(
        halo_out, halo_in, sent.at[13], got.at[8], sp=lax.rem(place + 1, sp)
    )

    @pl.when(place + 1 < sp)
    def _():
        halo_copy.start()

    late = delta_group(4, 4, 8)
    take(late, 2)
    advance(2, 0)
    take(late, 3)
    advance(3, 0)
    list(late)

    xin[0] = state_ref[...].astype(BF16)

    def x_copy(k):
        return remote(xin.at[0], xin.at[k], sent.at[12], got.at[7], sp=sp_at(0, k))

    for k in (2, 1, 3):
        x_copy(k).start()

    def unit_loop(t, carry):
        unit(t)
        return carry

    landed(wc.at[pl.ds(1, NY - 1), pl.ds(0, 96), :], got.at[2])
    w_beside().start()
    lax.fori_loop(0, chunks - 1, unit_loop, 0)

    def conv(t, carry):
        total = jnp.zeros((BLOCK, width), F32)
        for j in range(kernel):
            start = t * BLOCK + (halo - kernel + 1 + j)
            total = total + padded[pl.ds(start, BLOCK), :] * tapf_s[j : j + 1, :]
        filtered[at(t), :] = total
        first = jnp.sum(total, axis=1, keepdims=True)
        second = jnp.sum(total * total, axis=1, keepdims=True)
        turned = jnp.where(col_id == 0, first, jnp.where(col_id == 1, second, 0.0)).T
        sums_out[pl.ds(t, 1), :] = turned[0:1, :]
        sums_out[pl.ds(t + 8, 1), :] = turned[1:2, :]
        return carry

    lax.fori_loop(1, chunks, conv, 0)

    @pl.when(place >= 1)
    def _():
        halo_copy.wait_recv()

    @pl.when(place < 1)
    def _():
        halo_in[...] = jnp.zeros(halo_in.shape, BF16)

    padded[:halo, :] = halo_in[...].astype(F32)
    conv(0, 0)

    def ln_copy(o, p):
        i = 2 * o + p - 1
        return remote(sums_out, sums_in.at[i], sent.at[14], got.at[9], tp=tp_at(o, p))

    others = [(2, 0), (2, 1), (1, 0), (1, 1), (3, 0), (3, 1), (0, 1)]
    for o, p in others:
        ln_copy(o, p).start()
    landed(wd.at[pl.ds(0, 2), pl.ds(0, BLOCK), :], got.at[5])
    d_on_right().start()
    d_on_left().start()
    for d in (0, 1, 3):
        d_beside(d).start()

    landed(xin.at[pl.ds(1, NX - 1)], got.at[7])

    def piece(i):
        return xin[lax.rem(x - i + NX, NX)]

    p0, p1, p2, p3 = (piece(i) for i in range(NX))
    w2 = compose(p1, p0)
    pair = compose(p3, p2)
    group = compose(pair, w2)
    w3 = compose(p2, w2)
    inner = jnp.where(
        x == 0, ident, jnp.where(x == 1, p0.astype(F32), jnp.where(x == 2, w2, w3))
    ).astype(BF16)
    zs[0] = group.astype(BF16)

    def z_copy(i, b):
        cut = pl.ds(b * width, width)
        return remote(
            zs.at[i, :, cut], zr.at[i, :, cut],
            z_send.at[2 * i + b], z_recv.at[2 * i + b], sp=sp_at(i + 1, 0),
        )

    last_copy = remote(zs4, zr4, z_send.at[4], z_recv.at[4], sp=sp_at(4, 0))

    def z_start(i, b):
        @pl.when(z + i + 1 < NZ)
        def _():
            z_copy(i, b).start()

    def z_wait(i, b):
        @pl.when(z >= i + 1)
        def _():
            z_copy(i, b).wait_recv()

    z_start(0, 1)
    z_start(0, 0)

    for i in range(2):

        @pl.when(z < i + 1)
        def _(i=i):
            zr[i] = ident.astype(BF16)

    @pl.when(z < 4)
    def _():
        zr4[...] = jnp.zeros(zr4.shape, BF16)

    settle(full.at[:, columns(me)], 0)
    settle(full.at[:, columns(me)], 1)
    settle(full.at[pl.ds(0, rows // 2), columns(me)], 2)
    settle(full.at[pl.ds(0, rows // 2), columns(me)], 3)
    settle(full.at[:, pl.ds(0, NY * part)], 4)
    settle(wc.at[0, pl.ds(0, 3 * zrows), pl.ds(0, xcols)], 5)
    settle(wc.at[pl.ds(1, NY - 1), pl.ds(0, 7 * zrows), pl.ds(0, xcols)], 6)
    settle(wc.at[pl.ds(1, NY - 1), pl.ds(0, 96), :], 7)
    settle(xin.at[pl.ds(1, NX - 1)], 12)

    def left(i):
        return zs[i][:, :width]

    z_wait(0, 1)
    zs[1, :, width:] = (
        mm(left(0), zr[0, :, width:]) + zs[0, :, width:].astype(F32)
    ).astype(BF16)
    z_start(1, 1)
    z_wait(0, 0)
    e1 = zr[0]
    zs[1, :, :width] = mm(left(0), e1[:, :width]).astype(BF16)
    z_start(1, 0)

    landed(sums_in, got.at[9])
    loads["lng"].wait()
    loads["lns"].wait()
    loads["gain"].wait()
    sums = sums_out[...]
    for i in range(7):
        sums = sums + sums_in[i]
    sums = jnp.concatenate([sums, jnp.zeros((BLOCK - 16, BLOCK), F32)], axis=0).T
    channels = width * 2 * NY
    center_all = sums[:, 0:8] / channels
    variance = jnp.maximum(sums[:, 8:16] / channels - center_all * center_all, 0.0)
    scale_all = lax.rsqrt(variance + TINY_VAR)
    for t in range(chunks):
        here = slice(t * BLOCK, (t + 1) * BLOCK)
        normed = (filtered[here, :] - center_all[:, t : t + 1]) * scale_all[:, t : t + 1]
        normed = normed * lng_s[...] + lns_s[...]
        gate = proj[6, here, :].astype(F32)
        cm_s[here, :] = (jax.nn.silu(normed) * jax.nn.silu(gate)).astype(BF16)

    def c_copy(o, p):
        i = 2 * o + p - 1
        return remote(
            cm_s.at[at(tp_at(o, p)), :],
            in_c.at[(NY - o) % NY, :, pl.ds(p * width, width)],
            sent.at[15], got.at[10], tp=tp_at(o, p),
        )

    for o, p in others:
        c_copy(o, p).start()
    in_c[0, :, :width] = cm_s[at(me), :]
    z_wait(1, 1)
    zs4[...] = (mm(left(1), zr[1, :, width:]) + zs[1, :, width:].astype(F32)).astype(BF16)

    @pl.when(z + 4 < NZ)
    def _():
        last_copy.start()

    landed(wd.at[0, pl.ds(0, BLOCK), :], got.at[6])
    d_beside(2).start()
    z_wait(1, 0)
    e3 = compose(e1, zr[1])
    reach = compose(inner, e3)

    for t in range(chunks):
        here = slice(t * BLOCK, (t + 1) * BLOCK)
        gate_s[here, :] = gain_s[...] * jax.nn.silu(proj[3, here, :].astype(F32))

    w_beside().wait_recv()
    landed(dsend, got.at[10])
    step = 512
    cuts = out_ref.shape[1] // step

    def out_copy(n):
        cut = pl.ds(n * step, step)
        return pltpu.make_async_copy(out_ref.at[:, cut], out_hbm.at[:, cut], l_sem.at[0])

    for n in range(cuts):
        cut = slice(n * step, (n + 1) * step)
        total = jnp.zeros((BLOCK, step), F32)
        for d in range(NY):
            total = total + jnp.dot(in_c[d], wc[d, :, cut], preferred_element_type=F32)
        acc[:, cut] = total

    @pl.when(z >= 4)
    def _():
        last_copy.wait_recv()

    carried = (mm(reach[:, :width], zr4[...]) + reach[:, width:]).astype(BF16)

    def d_copy(o, p):
        i = 2 * o + p - 1
        return remote(
            dsend.at[i], in_d.at[(NY - o) % NY, :, pl.ds(p * width, width)],
            sent.at[16], got.at[0 if o == 0 else 11 if o == 2 else 12], tp=tp_at(o, p),
        )

    for batch in (others[:6], [(0, 1), (0, 0)]):
        places = [at(tp_at(o, p)) for o, p in batch]
        results = [outb_s[pos, :] + mm(outa_s[pos, :], carried) for pos in places]
        scales = [
            lax.rsqrt(jnp.mean(res * res, axis=-1, keepdims=True) + TINY_NORM) for res in results
        ]
        mixed = [
            (res * sc * gate_s[pos, :]).astype(BF16)
            for res, sc, pos in zip(results, scales, places)
        ]
        for (o, p), value in zip(batch, mixed):
            if o == 0 and p == 0:
                in_d[0, :, :width] = value
            else:
                dsend[2 * o + p - 1] = value
        for o, p in batch:
            if o or p:
                d_copy(o, p).start()

    landed(wd.at[:, pl.ds(0, BLOCK), :], got.at[4])
    for group_at, count, sem in (((0,), 1, 0), ((3, 1), 4, 12), ((2,), 2, 11)):
        landed(dsend.at[pl.ds(0, count)], got.at[sem])
        for n in range(cuts):
            cut = slice(n * step, (n + 1) * step)
            total = acc[:, cut]
            for d in group_at:
                total = total + jnp.dot(in_d[d], wd[d, :, cut], preferred_element_type=F32)
            if group_at == (2,):
                out_ref[:, cut] = total.astype(BF16)
                out_copy(n).start()
            else:
                acc[:, cut] = total

    settle(wc.at[:, pl.ds(0, BLOCK), :], 8)
    settle(wd.at[:, pl.ds(0, BLOCK), :], 9)
    settle(wd.at[pl.ds(0, 2), pl.ds(0, BLOCK), :], 10)
    settle(wd.at[0, pl.ds(0, BLOCK), :], 11)

    @pl.when(place + 1 < sp)
    def _():
        halo_copy.wait_send()

    for i in range(2):

        @pl.when(z + i + 1 < NZ)
        def _(i=i):
            z_copy(i, 0).wait_send()
            z_copy(i, 1).wait_send()

    @pl.when(z + 4 < NZ)
    def _():
        last_copy.wait_send()

    settle(sums_in, 14)
    settle(dsend, 15)
    settle(dsend, 16)
    pltpu.make_async_copy(out_ref, out_hbm, l_sem.at[0]).wait()


def local(
    tokens, w_query, w_key, w_value, w_delta_gate, w_glu_value, w_glu_gate, w_conv_gate,
    w_beta, w_decay, decay_log, head_gain, conv_taps, ln_gain, ln_shift, out_delta, out_conv,
):
    rows, part = tokens.shape
    depth, width = w_query.shape
    wide = out_delta.shape[1]
    heads = w_beta.shape[1]
    chunks = rows // BLOCK
    kernel = conv_taps.shape[0]
    halo = (kernel - 1 + 31) // 32 * 32
    hbm = pl.BlockSpec(memory_space=pltpu.HBM)
    dma = pltpu.SemaphoreType.DMA
    vm = pltpu.VMEM
    return pl.pallas_call(
        layer_kernel,
        out_shape=jax.ShapeDtypeStruct((BLOCK, wide), BF16),
        in_specs=[hbm] * 17,
        out_specs=hbm,
        scratch_shapes=[
            vm((BLOCK, wide), BF16),
            vm((rows, depth), BF16),
            vm((depth, 8 * width), BF16),
            vm((7, rows, width), BF16),
            vm((rows, width), F32),
            vm((heads, depth), BF16),
            vm((heads, depth), BF16),
            vm((1, heads), F32),
            vm((1, width), F32),
            vm((kernel, width), BF16),
            vm((32, width), F32),
            vm((1, width), F32),
            vm((1, width), F32),
            vm((NY, 2 * BLOCK, wide), BF16),
            vm((NY, 2 * BLOCK, wide), BF16),
            vm((chunks, 2 * BLOCK, width), BF16),
            vm((rows, width), F32),
            vm((rows, BLOCK), BF16),
            vm((chunks, width, BLOCK), BF16),
            vm((chunks, 8, BLOCK), F32),
            vm((width, 2 * width), F32),
            vm((rows, width), BF16),
            vm((rows, width), F32),
            vm((NX, width, 2 * width), BF16),
            vm((2, width, 2 * width), BF16),
            vm((2, width, 2 * width), BF16),
            vm((width, width), BF16),
            vm((width, width), BF16),
            vm((halo + rows, width), F32),
            vm((rows, width), F32),
            vm((halo, width), BF16),
            vm((halo, width), BF16),
            vm((16, BLOCK), F32),
            vm((7, 16, BLOCK), F32),
            vm((rows, width), BF16),
            vm((7, BLOCK, width), BF16),
            vm((NY, BLOCK, 2 * width), BF16),
            vm((NY, BLOCK, 2 * width), BF16),
            vm((BLOCK, wide), F32),
            vm((rows, width), F32),
            dma((11,)),
            dma((17,)),
            dma((chunks,)),
            dma((chunks,)),
            dma((chunks,)),
            dma((NZ - 1,)),
            dma((13,)),
            dma((5,)),
            dma((5,)),
        ],
        compiler_params=pltpu.CompilerParams(
            collective_id=0, has_side_effects=True, vmem_limit_bytes=60 * 1024 * 1024
        ),
        cost_estimate=pl.CostEstimate(
            flops=10_000_000_000, bytes_accessed=20_000_000, transcendentals=0
        ),
        name="layer",
    )(
        tokens, w_query, w_key, w_value, w_delta_gate, w_glu_value, w_glu_gate, w_conv_gate,
        w_beta.T, w_decay.T, decay_log[None, :], head_gain[None, :], conv_taps,
        ln_gain[None, :], ln_shift[None, :], out_delta, out_conv,
    )


def solution(mesh):
    return jax.shard_map(
        local,
        mesh=mesh,
        in_specs=(
            P("sp", "tp"), P(None, "tp"), P(None, "tp"), P(None, "tp"), P(None, "tp"),
            P(None, "tp"), P(None, "tp"), P(None, "tp"), P(), P(), P(), P(), P(None, "tp"),
            P("tp"), P("tp"), P("tp", None), P("tp", None),
        ),
        out_specs=P(("sp", "tp"), None),
        check_vma=False,
    )
```
